32 devices in a mesh: sp: 16 (over z, y, x), tp: 2 (over core).
Axes of the slice: x: 2, y: 2, z: 4, core: 2. Of those that a mesh axis runs over, the one named last changes fastest.
Arguments:
- tokens: bfloat16 [8192, 2048], P('sp', 'tp'), may hold values from -6 to 6
- input_gain: bfloat16 [2048], P('tp'), may hold values from 0.099609375 to 1.8984375
- query_weight: bfloat16 [2048, 1024], P(None, 'tp'), may hold values from -10 to 10
- key_weight: bfloat16 [2048, 1024], P(None, 'tp'), may hold values from -10 to 10
- value_weight: bfloat16 [2048, 1024], P(None, 'tp'), may hold values from -0.125 to 0.125
- pool_in_weight: bfloat16 [2048, 1024], P(None, 'tp'), may hold values from -0.125 to 0.125
- log_gates: float32 [8, 8192], P('tp'), may hold values from -8192 to 0, as said below
- pool_weight: bfloat16 [8, 128, 128], P('tp'), may hold values from -0.5 to 0.5
- pool_scale: float32 [1024], P('tp'), may hold values from 0.1 to 1.9
- attention_out: bfloat16 [1024, 2048], P('tp'), may hold values from -16 to 16
- pooling_out: bfloat16 [1024, 2048], P('tp'), may hold values from -16 to 16
- final_gain: float32 [2048], P('tp'), may hold values from 0.1 to 1.9
Outputs:
- layer_out: bfloat16 [8192, 2048], P('sp', 'tp')
The draws below stay inside these ranges and needn't reach their ends.
Inputs may be any that keep to these rules, and one draw needn't show every extreme that they name: `log_gates`: each row does not increase along positions.
All inputs are finite; a program needn't handle non-finite values.
Results may differ from the reference program's by a relative error of at most 0.015.
Values may be sent and summed in bfloat16 or wider, within the bound.
A program may use at most 128 MiB of HBM per device.

```python
import math
import jax
import jax.numpy as jnp
from jax import lax

D = 2048
HEAD = 128
ATT_HEADS = 8
POOL_GROUPS = 8
TOK_DEV = 512
TOKENS = 8192


def pair_bases(key):
    first = jnp.clip(jax.random.normal(jax.random.fold_in(key, 101), (D, ATT_HEADS * HEAD), jnp.float32), -4.0, 4.0)
    second = jnp.clip(jax.random.normal(jax.random.fold_in(key, 102), (D, ATT_HEADS * HEAD), jnp.float32), -4.0, 4.0)
    return (first, second)


def draw_query_weight(key, part):
    first, second = pair_bases(key)
    drawn = first
    return (drawn * D ** (-0.5)).astype(jnp.bfloat16)


def draw_key_weight(key, part):
    first, second = pair_bases(key)
    drawn = 3.0 * second
    return (drawn * D ** (-0.5)).astype(jnp.bfloat16)


def draw_log_gates(key, part):
    heads = ATT_HEADS
    order = jax.random.permutation(jax.random.fold_in(key, 31), heads)
    slow = order < heads // 2
    forget_span = jnp.exp(jax.random.uniform(jax.random.fold_in(key, 32), (heads,), jnp.float32, math.log(30.0), math.log(100.0)))
    starting_shift_amount = jnp.where(slow, 0.55 / TOKENS, 1.0 / forget_span)
    approximate_guess = jnp.exp(jax.random.uniform(jax.random.fold_in(key, 33), (heads, TOKENS), jnp.float32, -math.log(4.0), math.log(4.0)))
    blocks = jnp.exp(jax.random.uniform(jax.random.fold_in(key, 34), (heads, TOKENS // TOK_DEV), jnp.float32, -math.log(2.0), math.log(2.0)))
    tile_scaling_factor = jnp.repeat(blocks, TOK_DEV, axis=1)
    seat_indices = jax.random.randint(jax.random.fold_in(key, 35), (heads, 2), 0, TOKENS)
    objective_numbers = jnp.log(jax.random.uniform(jax.random.fold_in(key, 36), (heads, 2), jnp.float32, 0.5, 0.8))
    element_locations = jnp.arange(TOKENS, dtype=jnp.int32)
    segment_clusters = jnp.sum(jnp.where(element_locations[None, None, :] == seat_indices[:, :, None], objective_numbers[:, :, None], 0.0), axis=1)
    return jnp.cumsum(segment_clusters - starting_shift_amount[:, None] * approximate_guess * tile_scaling_factor, axis=1).astype(jnp.float32)


def rising_weight(key, rows, salt):
    noise = jnp.clip(jax.random.normal(jax.random.fold_in(key, salt), (rows, D), jnp.float32), -4.0, 4.0)
    highest = 10.0
    jitter = jnp.exp(jax.random.uniform(jax.random.fold_in(key, salt + 1), (D,), jnp.float32, -0.35, 0.35))
    rising = jnp.exp(math.log(highest) * jnp.arange(D, dtype=jnp.float32) / D) * jitter
    return (noise * rising[None, :] * rows ** (-0.5)).astype(jnp.bfloat16)


def draw_attention_out(key, part):
    return rising_weight(key, ATT_HEADS * HEAD, 41)


def draw_pooling_out(key, part):
    return rising_weight(key, POOL_GROUPS * HEAD, 51)


def levels(rng, dims, shards, low, largest):
    def one(dim, blocks):
        heights = jax.random.uniform(jax.random.fold_in(jax.random.fold_in(rng, 6), dim), (blocks,), jnp.float32, low / len(shards), largest / len(shards))
        return jnp.repeat(jnp.exp(heights), dims[dim] // blocks).reshape((-1,) + (1,) * (len(dims) - dim - 1))

    gain = one(*shards[0])
    for cut in shards[1:]:
        gain = gain * one(*cut)
    return gain


def bell_draw(stream_key, shape, scale, bound, split=(), kind=jnp.bfloat16):
    level = levels(stream_key, shape, split, -0.22, 0.18) if split else 1.0
    values = jax.random.normal(stream_key, shape, jnp.float32) * scale * level
    return jnp.minimum(jnp.maximum(values, -bound), bound).astype(kind)


def setup_inputs(seed: int = 0) -> dict:
    splits = jax.random.split(jax.random.key(seed), 13)
    tokens = bell_draw(splits[0], (TOKENS, D), 1.0, 6.0, ((0, 16), (1, 2)))
    input_gain = jnp.clip(1.0 + 0.18 * jax.random.normal(splits[1], (D,), jnp.float32), 0.099609375, 1.8984375).astype(jnp.bfloat16)
    query_weight = draw_query_weight(jax.random.fold_in(splits[12], 71), 0)
    key_weight = draw_key_weight(jax.random.fold_in(splits[12], 71), 0)
    value_weight = bell_draw(splits[4], (D, ATT_HEADS * HEAD), D ** -0.5, 0.125, ((1, 2),))
    pool_in_weight = bell_draw(splits[5], (D, POOL_GROUPS * HEAD), D ** -0.5, 0.125, ((1, 2),))
    log_gates = draw_log_gates(jax.random.fold_in(splits[12], 71), 0)
    pool_weight = bell_draw(splits[7], (POOL_GROUPS, HEAD, HEAD), HEAD ** -0.5, 0.5, ((0, 2),))
    pool_scale = jnp.clip(1.0 + 0.18 * jax.random.normal(splits[8], (POOL_GROUPS * HEAD,), jnp.float32), 0.1, 1.9)
    attention_out = draw_attention_out(jax.random.fold_in(splits[12], 71), 0)
    pooling_out = draw_pooling_out(jax.random.fold_in(splits[12], 71), 0)
    final_gain = jnp.clip(1.0 + 0.18 * jax.random.normal(splits[11], (D,), jnp.float32), 0.1, 1.9)
    return {"tokens": tokens, "input_gain": input_gain, "query_weight": query_weight, "key_weight": key_weight, "value_weight": value_weight, "pool_in_weight": pool_in_weight, "log_gates": log_gates, "pool_weight": pool_weight, "pool_scale": pool_scale, "attention_out": attention_out, "pooling_out": pooling_out, "final_gain": final_gain}


epsilon = 1e-06

def attention(query, keys, values, log_gates):
    total_rows = query.shape[0]
    heads = log_gates.shape[0]
    head_size = query.shape[1] // heads
    block = math.gcd(total_rows, 256)
    query_blocks = query.reshape(total_rows // block, block, heads, head_size).astype(jnp.float32)
    keys_whole = keys.reshape(total_rows, heads, head_size).astype(jnp.float32)
    values_whole = values.reshape(total_rows, heads, head_size).astype(jnp.float32)
    key_rows = jnp.arange(total_rows, dtype=jnp.int32)

    def one_block(args):
        query_block, first = args
        query_gate = lax.dynamic_slice_in_dim(log_gates, first, block, 1).T
        scores = jnp.einsum('thd,shd->ths', query_block, keys_whole) * head_size ** (-0.5)
        scores = scores + query_gate[:, :, None] - log_gates[None, :, :]
        rows = first + jnp.arange(block, dtype=jnp.int32)
        allowed = (rows[:, None] >= key_rows[None, :])[:, None, :]
        scores = jnp.where(allowed, scores, -jnp.inf)
        row_max = lax.optimization_barrier(jnp.max(scores, axis=2, keepdims=True))
        weights = jnp.exp(scores - row_max)
        totals = lax.optimization_barrier(jnp.sum(weights, axis=2))
        rounded = lax.optimization_barrier(weights.astype(jnp.bfloat16)).astype(jnp.float32)
        result = jnp.einsum('ths,shd->thd', rounded, values_whole) / totals[:, :, None]
        return result.astype(jnp.bfloat16)
    block_starts = jnp.arange(total_rows // block, dtype=jnp.int32) * block
    result = lax.map(one_block, (query_blocks, block_starts))
    return result.reshape(total_rows, heads * head_size)

def pooling(pool_input, pool_weight, pool_scale):
    total_rows, width = pool_input.shape
    groups = pool_weight.shape[0]
    head_size = pool_weight.shape[1]
    widened = pool_input.astype(jnp.float32)
    running = jnp.cumsum(widened, axis=0)
    padded = jnp.concatenate([jnp.zeros((1, width), jnp.float32), running], axis=0)
    rows = jnp.arange(total_rows, dtype=jnp.int32)[:, None]
    column = jnp.arange(width, dtype=jnp.int32)
    window = jnp.left_shift(jnp.full((width,), 2, jnp.int32), column // head_size % 4)
    lower = jnp.maximum(rows + 1 - window[None, :], 0).astype(jnp.int32)
    counts = (rows + 1 - lower).astype(jnp.float32)
    window_sum = running - jnp.take_along_axis(padded, lower, axis=0)
    departure = (window_sum / counts - widened).astype(jnp.bfloat16)
    mapped = jnp.einsum('tgc,gcd->tgd', departure.reshape(total_rows, groups, head_size).astype(jnp.float32), pool_weight.astype(jnp.float32))
    return (mapped.reshape(total_rows, width) * pool_scale).astype(jnp.bfloat16)

def reference(tokens, input_gain, query_weight, key_weight, value_weight, pool_in_weight, log_gates, pool_weight, pool_scale, attention_out, pooling_out, final_gain):
    widened = tokens.astype(jnp.float32)
    inverse = lax.rsqrt(lax.optimization_barrier(jnp.mean(widened * widened, axis=1)) + epsilon)[:, None]
    scaled = (widened * input_gain.astype(jnp.float32)).astype(jnp.bfloat16)

    def project(weight):
        return (jnp.dot(scaled, weight, preferred_element_type=jnp.float32) * inverse).astype(jnp.bfloat16)
    attended = attention(project(query_weight), project(key_weight), project(value_weight), log_gates)
    pooled = pooling(project(pool_in_weight), pool_weight, pool_scale)
    mixed = jnp.dot(attended, attention_out, preferred_element_type=jnp.float32) + jnp.dot(pooled, pooling_out, preferred_element_type=jnp.float32)
    out_inverse = lax.rsqrt(lax.optimization_barrier(jnp.mean(mixed * mixed, axis=1)) + epsilon)[:, None]
    return (mixed * out_inverse * final_gain).astype(jnp.bfloat16)
```

```python
import functools

import jax
import jax.numpy as jnp
from jax import lax
from jax.experimental import pallas as pl
from jax.experimental.pallas import tpu as pltpu
from jax.sharding import PartitionSpec as P


WINDOW_MAX = 16
LANES = 128
LOG2E = 1.4426950408889634

very_low = -1e30
epsilon = 1e-06


def passed_along(block, axis, distance):
    devices = range(lax.axis_size(axis))
    route = [(i - distance, i) for i in devices if i - distance in devices]
    return lax.ppermute(block, axis, route)


def swapped(block, axis, offset):
    return lax.ppermute(block, axis, [(i, i ^ offset) for i in range(lax.axis_size(axis))])


def attend_kernel(first, last, heads, head_size, chunk, mode_ref, start_ref, *refs):
    if first:
        q_ref, kv_ref, gate_ref, acc_out, ml_out = refs
    else:
        q_ref, kv_ref, gate_ref, acc_in, ml_in, acc_out, ml_out = refs
    slot = pl.program_id(0)
    rows = q_ref.shape[1]
    keys = kv_ref.shape[0]
    width = heads * head_size
    lane = lax.broadcasted_iota(jnp.int32, (chunk, LANES), 1)

    def state_of(r, h):
        if first:
            return None
        ml = ml_in[0, r : r + chunk, :]
        columns = slice(h * head_size, (h + 1) * head_size)
        return (ml[:, h : h + 1], ml[:, heads + h : heads + h + 1], acc_in[0, r : r + chunk, columns])

    def store(r, h, ml, state):
        columns = slice(h * head_size, (h + 1) * head_size)
        high, total, summed = state
        if last:
            safe = jnp.where(total > 0.0, total, 1.0)
            acc_out[0, r : r + chunk, columns] = (summed / safe).astype(acc_out.dtype)
            level = jnp.where(total > 0.0, high + jnp.log2(safe), very_low)
            return jnp.where(lane == h, level, ml)
        acc_out[0, r : r + chunk, columns] = summed
        return jnp.where(lane == h, high, jnp.where(lane == heads + h, total, ml))

    def compute(diagonal):
        for r in range(0, rows, chunk):
            ml = jnp.zeros((chunk, LANES), jnp.float32)
            span = min(r + chunk, keys) if diagonal else keys
            for h in range(heads):
                columns = slice(h * head_size, (h + 1) * head_size)
                q = q_ref[0, r : r + chunk, columns]
                k = kv_ref[:span, columns]
                v = kv_ref[:span, width + h * head_size : width + (h + 1) * head_size]
                bias = (start_ref[slot * heads + h] - gate_ref[h : h + 1, :span]) * LOG2E
                s = lax.dot_general(q, k, (((1,), (1,)), ((), ())), preferred_element_type=jnp.float32)
                s = s + bias
                if diagonal:
                    row = r + lax.broadcasted_iota(jnp.int32, s.shape, 0)
                    s = jnp.where(row >= lax.broadcasted_iota(jnp.int32, s.shape, 1), s, very_low)
                old = state_of(r, h)
                high = jnp.max(s, axis=1, keepdims=True)
                if old is not None:
                    high = jnp.maximum(high, old[0])
                p = jnp.exp2(s - high)
                total = jnp.sum(p, axis=1, keepdims=True)
                summed = jnp.dot(p.astype(jnp.bfloat16), v, preferred_element_type=jnp.float32)
                if old is not None:
                    factor = jnp.exp2(old[0] - high)
                    total = total + factor * old[1]
                    summed = summed + factor * old[2]
                ml = store(r, h, ml, (high, total, summed))
            ml_out[0, r : r + chunk, :] = ml

    if first:
        pl.when(slot == 0)(lambda: compute(True))

        @pl.when((slot > 0) & (mode_ref[slot] > 0))
        def _():
            compute(False)

    else:

        @pl.when(mode_ref[slot] > 0)
        def _():
            compute(False)

    @pl.when((mode_ref[slot] == 0) & ((slot > 0) | (not first)))
    def _():
        for r in range(0, rows, chunk):
            ml = jnp.zeros((chunk, LANES), jnp.float32)
            for h in range(heads):
                old = state_of(r, h)
                if old is None:
                    old = (
                        jnp.full((chunk, 1), very_low, jnp.float32),
                        jnp.zeros((chunk, 1), jnp.float32),
                        jnp.zeros((chunk, head_size), jnp.float32),
                    )
                ml = store(r, h, ml, old)
            ml_out[0, r : r + chunk, :] = ml


def attend_step(mode, starts, queries, pair, gates, state, last, head_size):
    slots, rows, width = queries.shape
    heads = width // head_size
    first = state is None
    chunk = min(rows, 256)
    by_slot = lambda g, *_: (g, 0, 0)
    whole = lambda g, *_: (0, 0)
    in_specs = [
        pl.BlockSpec((1, rows, width), by_slot),
        pl.BlockSpec(pair.shape, whole),
        pl.BlockSpec(gates.shape, whole),
    ]
    state_specs = [pl.BlockSpec((1, rows, width), by_slot), pl.BlockSpec((1, rows, LANES), by_slot)]
    if not first:
        in_specs = in_specs + state_specs
    keys = pair.shape[0]
    return pl.pallas_call(
        functools.partial(attend_kernel, first, last, heads, head_size, chunk),
        out_shape=(
            jax.ShapeDtypeStruct((slots, rows, width), jnp.bfloat16 if last else jnp.float32),
            jax.ShapeDtypeStruct((slots, rows, LANES), jnp.float32),
        ),
        grid_spec=pltpu.PrefetchScalarGridSpec(
            num_scalar_prefetch=2, grid=(slots,), in_specs=in_specs, out_specs=state_specs
        ),
        compiler_params=pltpu.CompilerParams(dimension_semantics=("arbitrary",)),
        cost_estimate=pl.CostEstimate(
            flops=8 * slots * rows * keys * width,
            bytes_accessed=12 * slots * rows * width,
            transcendentals=slots * rows * keys * heads,
        ),
    )(mode, starts, queries, pair, gates, *(() if first else state))


MESH = pl.DeviceIdType.MESH
SUB_ROWS = 128


def exchange_kernel(
    planes, seats, q_ref, k_ref, v_ref, gate_ref, out_ref,
    keys, values, queries, results, acc, high,
    z_send, z_recv, x_send, x_recv, y_send, y_recv, r_send, r_recv, o_send, o_recv,
):
    rows, head_size = queries.shape[1:]
    me = lax.axis_index("sp")
    plane, seat = me // seats, me % seats
    across = seat + 1 - 2 * (seat % 2)
    along = seat + 2 - 4 * (seat // 2)
    far = 3 - seat

    def device(p, s):
        return {"sp": p * seats + s}

    def block_rows(p, s):
        return pl.ds(pl.multiple_of((p * seats + s) * rows, rows), rows)

    def columns(p):
        return pl.ds(pl.multiple_of(p * head_size, head_size), head_size)

    def key_at(p, s):
        return keys.at[block_rows(p, s), :]

    def value_at(p, s):
        return values.at[block_rows(p, s), pl.ds(0, head_size)]

    def copy(source, target, send, recv, p, s):
        return pltpu.make_async_remote_copy(
            src_ref=source, dst_ref=target, send_sem=send, recv_sem=recv,
            device_id=device(p, s), device_id_type=MESH,
        )

    barrier = pltpu.get_barrier_semaphore()
    for d in range(1, planes):
        pl.semaphore_signal(barrier, inc=1, device_id=device((plane + d) % planes, seat), device_id_type=MESH)
    for s in (across, along):
        pl.semaphore_signal(barrier, inc=1, device_id=device(plane, s), device_id_type=MESH)
    pl.semaphore_wait(barrier, planes + 1)

    def from_plane(d):
        return (plane + planes - d) % planes

    def query_copy(d):
        to = (plane + d) % planes
        return copy(q_ref.at[:, columns(to)], queries.at[plane], z_send.at[0, d], z_recv.at[0, d], to, seat)

    def pair_copies(d):
        to = (plane + d) % planes
        return (
            copy(k_ref.at[:, columns(to)], key_at(plane, seat), z_send.at[1, d], z_recv.at[1, d], to, seat),
            copy(v_ref.at[:, columns(to)], value_at(plane, seat), z_send.at[2, d], z_recv.at[2, d], to, seat),
        )

    def spread(d, own):
        p = from_plane(d)
        k = k_ref.at[:, columns(plane)] if own else key_at(p, seat)
        v = v_ref.at[:, columns(plane)] if own else value_at(p, seat)
        return (
            copy(k, key_at(p, seat), x_send.at[0, d], x_recv.at[0, d], plane, across),
            copy(v, value_at(p, seat), y_send.at[1, d], y_recv.at[1, d], plane, along),
            copy(v, value_at(p, seat), x_send.at[1, d], x_recv.at[1, d], plane, across),
            copy(k, key_at(p, seat), y_send.at[0, d], y_recv.at[0, d], plane, along),
        )

    def relays(d):
        p = from_plane(d)
        return (
            copy(key_at(p, across), key_at(p, across), r_send.at[0, d], r_recv.at[0, d], plane, along),
            copy(value_at(p, along), value_at(p, along), r_send.at[1, d], r_recv.at[1, d], plane, across),
        )

    def arrival(target, recv):
        pltpu.make_async_remote_copy(
            src_ref=target, dst_ref=target, send_sem=z_send.at[0, 0], recv_sem=recv,
            device_id=device(plane, across), device_id_type=MESH,
        ).wait_recv()

    for d in range(1, planes):
        query_copy(d).start()
    for d in range(1, planes):
        for c in pair_copies(d):
            c.start()
    for c in spread(0, True):
        c.start()

    values[:, head_size:] = jnp.ones((values.shape[0], head_size), values.dtype)
    keys[block_rows(plane, seat), :] = k_ref[:, columns(plane)]
    values[block_rows(plane, seat), :head_size] = v_ref[:, columns(plane)]
    queries[plane] = q_ref[:, columns(plane)]
    acc[...] = jnp.zeros_like(acc)
    high[...] = jnp.full_like(high, very_low)

    def forward(d):
        p = from_plane(d)
        arrival(key_at(p, seat), z_recv.at[1, d])
        arrival(value_at(p, seat), z_recv.at[2, d])
        for c in spread(d, False):
            c.start()

    def relay(d):
        p = from_plane(d)
        to_along, to_across = relays(d)
        arrival(key_at(p, across), x_recv.at[0, d])
        to_along.start()
        arrival(value_at(p, along), y_recv.at[1, d])
        to_across.start()

    def settle(d):
        p = from_plane(d)
        arrival(value_at(p, across), x_recv.at[1, d])
        arrival(key_at(p, along), y_recv.at[0, d])
        arrival(key_at(p, far), r_recv.at[0, d])
        arrival(value_at(p, far), r_recv.at[1, d])

    span = seats * rows

    def head_gates(here):
        block = gate_ref[:, here]
        mine = lax.broadcasted_iota(jnp.int32, block.shape, 0) == plane
        return jnp.sum(jnp.where(mine, block, 0.0), axis=0, keepdims=True)

    def update(i, p, masked):
        here = pl.ds(pl.multiple_of(p * span, span), span)
        k = keys[here, :]
        v = values[here, :]
        gates = head_gates(here)
        start = head_gates(pl.ds(pl.multiple_of((i * seats + seat) * rows, rows), LANES))[:, :1]
        bias = (start - gates) * LOG2E
        scores = []
        for r in range(0, rows, SUB_ROWS):
            q = queries[i, r : r + SUB_ROWS, :]
            s = lax.dot_general(q, k, (((1,), (1,)), ((), ())), preferred_element_type=jnp.float32) + bias
            if masked:
                row = seat * rows + r + lax.broadcasted_iota(jnp.int32, s.shape, 0)
                s = jnp.where(row >= lax.broadcasted_iota(jnp.int32, s.shape, 1), s, very_low)
            scores.append(s)
        for n, r in enumerate(range(0, rows, SUB_ROWS)):
            s = scores[n]
            at = pl.ds(r, SUB_ROWS)
            old = high[i, at, :]
            new = jnp.maximum(old, jnp.max(s, axis=1, keepdims=True))
            p_ = jnp.exp2(s - new[:, :1]).astype(jnp.bfloat16)
            factor = jnp.exp2(old - new)
            summed = jnp.dot(p_, v, preferred_element_type=jnp.float32)
            acc[i, at, :] = acc[i, at, :] * jnp.concatenate([factor, factor], axis=1) + summed
            high[i, at, :] = new

    def finished(t):
        to = (plane + t) % planes
        return copy(results.at[to], out_ref.at[:, columns(plane)], o_send.at[t], o_recv.at[t], to, seat)

    relay(0)
    for d in range(1, planes):
        p = from_plane(d)
        arrival(queries.at[p], z_recv.at[0, d])

    def step(d, carry):
        @pl.when(d > 0)
        def _():
            relay(d)

        @pl.when(d < planes - 1)
        def _():
            forward(d + 1)

        settle(d)
        p = from_plane(d)

        def one(t, carry):
            i = (plane + t) % planes

            @pl.when(i > p)
            def _():
                update(i, p, False)

            @pl.when(i == p)
            def _():
                update(i, p, True)

            @pl.when(d == planes - 1)
            def _():
                result = (acc[i, :, :head_size] / acc[i, :, head_size:]).astype(jnp.bfloat16)

                @pl.when(t < planes)
                def _():
                    results[i] = result
                    finished(t).start()

                @pl.when(t == planes)
                def _():
                    out_ref[:, columns(plane)] = result

            return carry

        lax.fori_loop(1, planes + 1, one, 0)
        return carry

    lax.fori_loop(0, planes, step, 0)
    for t in range(1, planes):
        query_copy(t).wait_send()
        for c in pair_copies(t):
            c.wait_send()
    for c in spread(0, True):
        c.wait_send()
    for t in range(1, planes):
        for c in spread(t, False):
            c.wait_send()
    for t in range(planes):
        for c in relays(t):
            c.wait_send()
    for t in range(1, planes):
        finished(t).wait_send()
        arrival(out_ref.at[:, columns(from_plane(t))], o_recv.at[t])


def exchange_attend(query, keys, values, log_gates):
    rows, width = query.shape
    planes = log_gates.shape[0]
    seats = lax.axis_size("sp") // planes
    head_size = width // planes
    blocks = planes * seats
    dma = pltpu.SemaphoreType.DMA
    pairs = blocks * (blocks + 1) // 2
    return pl.pallas_call(
        functools.partial(exchange_kernel, planes, seats),
        out_shape=jax.ShapeDtypeStruct((rows, width), jnp.bfloat16),
        in_specs=[pl.BlockSpec(memory_space=pltpu.VMEM)] * 4,
        out_specs=pl.BlockSpec(memory_space=pltpu.VMEM),
        scratch_shapes=[
            pltpu.VMEM((blocks * rows, head_size), jnp.bfloat16),
            pltpu.VMEM((blocks * rows, 2 * head_size), jnp.bfloat16),
            pltpu.VMEM((planes, rows, head_size), jnp.bfloat16),
            pltpu.VMEM((planes, rows, head_size), jnp.bfloat16),
            pltpu.VMEM((planes, rows, 2 * head_size), jnp.float32),
            pltpu.VMEM((planes, rows, LANES), jnp.float32),
            dma((3, planes)), dma((3, planes)),
            dma((2, planes)), dma((2, planes)),
            dma((2, planes)), dma((2, planes)),
            dma((2, planes)), dma((2, planes)),
            dma((planes,)), dma((planes,)),
        ],
        compiler_params=pltpu.CompilerParams(
            collective_id=0, has_side_effects=True, vmem_limit_bytes=48 * 2**20
        ),
        cost_estimate=pl.CostEstimate(
            flops=4 * pairs * rows * rows * head_size,
            bytes_accessed=2 * 4 * rows * width,
            transcendentals=pairs * rows * rows,
        ),
    )(query, keys, values, log_gates)


def ring_attend(query, keys, values, log_gates):
    tok_rows = query.shape[0]
    heads = log_gates.shape[0]
    head_size = query.shape[1] // heads
    devices = lax.axis_size("sp")
    side = 1
    while (2 * side) ** 2 <= devices and devices % (2 * side) == 0:
        side = 2 * side
    planes = devices // side
    sequence_index = lax.axis_index("sp")
    plane = sequence_index // side
    seat = sequence_index % side
    pair = jnp.concatenate([keys, values], axis=1)
    pairs = [pair]
    for _ in range(1, planes):
        pairs.append(passed_along(pairs[-1], "sp", side))
    queries = jnp.stack([query] + [swapped(query, "sp", g) for g in range(1, side)])
    seats = seat ^ jnp.arange(side, dtype=jnp.int32)
    starts = jnp.stack(
        [
            lax.dynamic_slice_in_dim(log_gates, (plane * side + (seat ^ g)) * tok_rows, 1, 1)[:, 0]
            for g in range(side)
        ]
    ).reshape(-1)
    state = None
    for k in range(planes):
        source = jnp.maximum(sequence_index - k * side, seat)
        gates = lax.dynamic_slice_in_dim(log_gates, source * tok_rows, tok_rows, 1)
        if k == 0:
            mode = (seats > seat).astype(jnp.int32)
        else:
            mode = jnp.full((side,), plane >= k, jnp.int32)
        state = attend_step(
            mode, starts, queries, pairs[k], gates, state, k == planes - 1, head_size
        )
    partial, level = state
    level = level[:, :, :heads]
    shares = [partial[0]] + [swapped(partial[g], "sp", g) for g in range(1, side)]
    tall = jnp.transpose(level, (0, 2, 1))
    levels = jnp.stack([tall[0]] + [swapped(tall[g], "sp", g) for g in range(1, side)])
    portion = jnp.exp2(levels - jnp.max(levels, axis=0, keepdims=True))
    portion = portion / jnp.sum(portion, axis=0, keepdims=True)
    portion = jnp.transpose(portion, (0, 2, 1))
    attended = 0.0
    for g in range(side):
        attended = attended + shares[g].astype(jnp.float32) * jnp.repeat(portion[g], head_size, axis=1)
    return attended.astype(jnp.bfloat16)


def gathered(block, axis):
    if lax.axis_size(axis) != 2:
        return lax.all_gather(block, axis, axis=1, tiled=True)
    other = swapped(block, axis, 1)
    lower = lax.axis_index(axis) == 0
    return jnp.concatenate([jnp.where(lower, block, other), jnp.where(lower, other, block)], axis=1)


def body(
    tokens,
    input_gain,
    query_weight,
    key_weight,
    value_weight,
    pool_in_weight,
    log_gates,
    pool_weight,
    pool_scale,
    attention_out,
    pooling_out,
    final_gain,
):
    tok_rows = tokens.shape[0]
    width = query_weight.shape[0]
    groups = pool_weight.shape[0]
    head_size = pool_weight.shape[1]
    heads = log_gates.shape[0]
    pool_width = pool_in_weight.shape[1]
    devices = lax.axis_size("sp")
    shards = lax.axis_size("tp")
    sequence_index = lax.axis_index("sp")
    first_row = sequence_index * tok_rows

    part = gathered(tokens, "tp")
    gain_part = gathered(input_gain.reshape(1, -1), "tp")
    widened = part.astype(jnp.float32)
    scaled = (widened * gain_part.astype(jnp.float32)).astype(jnp.bfloat16)

    def product(weight):
        return jnp.dot(scaled, weight, preferred_element_type=jnp.float32)

    inverse = lax.rsqrt(jnp.sum(widened * widened, axis=1) / width + epsilon)[:, None]
    keys = (product(key_weight) * inverse).astype(jnp.bfloat16)
    values = (product(value_weight) * inverse).astype(jnp.bfloat16)
    query = (product(query_weight) * (inverse * (LOG2E * head_size ** (-0.5)))).astype(jnp.bfloat16)
    pool_input = (product(pool_in_weight) * inverse).astype(jnp.bfloat16)
    rim = passed_along(pool_input[tok_rows - (WINDOW_MAX - 1) :], "sp", 1)

    spread = heads > 1 and devices == 4 * heads
    if spread:
        attended = exchange_attend(query, keys, values, log_gates)
    else:
        attended = ring_attend(query, keys, values, log_gates)

    extended = jnp.concatenate([rim, pool_input], axis=0).astype(jnp.float32)
    column = jnp.arange(pool_width, dtype=jnp.int32)
    group_number = lax.axis_index("tp") * groups + column // head_size
    window = jnp.left_shift(jnp.full((pool_width,), 2, jnp.int32), group_number % 4)
    sums = extended
    span = 1
    chosen = jnp.zeros((tok_rows, pool_width), jnp.float32)
    for _ in range(4):
        sums = sums[span:] + sums[:-span]
        span = span * 2
        offset_rows = WINDOW_MAX - span
        chosen = jnp.where(window[None, :] == span, sums[offset_rows : offset_rows + tok_rows], chosen)
    element_locations = first_row + jnp.arange(tok_rows, dtype=jnp.int32)
    counts = jnp.minimum(window[None, :], element_locations[:, None] + 1).astype(jnp.float32)
    departure = (chosen / counts - pool_input.astype(jnp.float32)).astype(jnp.bfloat16)
    mapped = jnp.concatenate(
        [
            jnp.dot(
                departure[:, g * head_size : (g + 1) * head_size],
                pool_weight[g],
                preferred_element_type=jnp.float32,
            )
            for g in range(groups)
        ],
        axis=1,
    )
    pooled = (mapped * pool_scale).astype(jnp.bfloat16)
    pooled_part = jnp.dot(pooled, pooling_out, preferred_element_type=jnp.float32)
    whole = jnp.dot(attended, attention_out, preferred_element_type=jnp.float32) + pooled_part
    if shards == 2:
        half = width // 2
        lower = lax.axis_index("tp") == 0
        sent = jnp.where(lower, whole[:, half:], whole[:, :half]).astype(jnp.bfloat16)
        kept = jnp.where(lower, whole[:, :half], whole[:, half:])
        mixed = kept + swapped(sent, "tp", 1).astype(jnp.float32)
        squares = jnp.sum(mixed * mixed, axis=1)
        squares = squares + swapped(squares, "tp", 1)
    else:
        mixed = lax.psum_scatter(
            whole.astype(jnp.bfloat16), "tp", scatter_dimension=1, tiled=True
        ).astype(jnp.float32)
        squares = lax.psum(jnp.sum(mixed * mixed, axis=1), "tp")
    out_inverse = lax.rsqrt(squares / width + epsilon)
    return (mixed * out_inverse[:, None] * final_gain[None, :]).astype(jnp.bfloat16)


def solution(mesh):
    return jax.shard_map(
        body,
        mesh=mesh,
        in_specs=(
            P("sp", "tp"),
            P("tp"),
            P(None, "tp"),
            P(None, "tp"),
            P(None, "tp"),
            P(None, "tp"),
            P("tp", None),
            P("tp", None, None),
            P("tp"),
            P("tp", None),
            P("tp", None),
            P("tp"),
        ),
        out_specs=P("sp", "tp"),
        check_vma=False,
    )
```

```python
import functools

import jax
import jax.numpy as jnp
from jax import lax
from jax.experimental import pallas as pl
from jax.experimental.pallas import tpu as pltpu
from jax.sharding import PartitionSpec as P


WINDOW_MAX = 16
LANES = 128
LOG2E = 1.4426950408889634

very_low = -1e30
epsilon = 1e-06


def passed_along(block, axis, distance):
    devices = range(lax.axis_size(axis))
    route = [(i - distance, i) for i in devices if i - distance in devices]
    return lax.ppermute(block, axis, route)


def swapped(block, axis, offset):
    return lax.ppermute(block, axis, [(i, i ^ offset) for i in range(lax.axis_size(axis))])


def attend_kernel(first, last, heads, head_size, chunk, mode_ref, start_ref, *refs):
    if first:
        q_ref, kv_ref, gate_ref, acc_out, ml_out = refs
    else:
        q_ref, kv_ref, gate_ref, acc_in, ml_in, acc_out, ml_out = refs
    slot = pl.program_id(0)
    rows = q_ref.shape[1]
    keys = kv_ref.shape[0]
    width = heads * head_size
    lane = lax.broadcasted_iota(jnp.int32, (chunk, LANES), 1)

    def state_of(r, h):
        if first:
            return None
        ml = ml_in[0, r : r + chunk, :]
        columns = slice(h * head_size, (h + 1) * head_size)
        return (ml[:, h : h + 1], ml[:, heads + h : heads + h + 1], acc_in[0, r : r + chunk, columns])

    def store(r, h, ml, state):
        columns = slice(h * head_size, (h + 1) * head_size)
        high, total, summed = state
        if last:
            safe = jnp.where(total > 0.0, total, 1.0)
            acc_out[0, r : r + chunk, columns] = (summed / safe).astype(acc_out.dtype)
            level = jnp.where(total > 0.0, high + jnp.log2(safe), very_low)
            return jnp.where(lane == h, level, ml)
        acc_out[0, r : r + chunk, columns] = summed
        return jnp.where(lane == h, high, jnp.where(lane == heads + h, total, ml))

    def compute(diagonal):
        for r in range(0, rows, chunk):
            ml = jnp.zeros((chunk, LANES), jnp.float32)
            span = min(r + chunk, keys) if diagonal else keys
            for h in range(heads):
                columns = slice(h * head_size, (h + 1) * head_size)
                q = q_ref[0, r : r + chunk, columns]
                k = kv_ref[:span, columns]
                v = kv_ref[:span, width + h * head_size : width + (h + 1) * head_size]
                bias = (start_ref[slot * heads + h] - gate_ref[h : h + 1, :span]) * LOG2E
                s = lax.dot_general(q, k, (((1,), (1,)), ((), ())), preferred_element_type=jnp.float32)
                s = s + bias
                if diagonal:
                    row = r + lax.broadcasted_iota(jnp.int32, s.shape, 0)
                    s = jnp.where(row >= lax.broadcasted_iota(jnp.int32, s.shape, 1), s, very_low)
                old = state_of(r, h)
                high = jnp.max(s, axis=1, keepdims=True)
                if old is not None:
                    high = jnp.maximum(high, old[0])
                p = jnp.exp2(s - high)
                total = jnp.sum(p, axis=1, keepdims=True)
                summed = jnp.dot(p.astype(jnp.bfloat16), v, preferred_element_type=jnp.float32)
                if old is not None:
                    factor = jnp.exp2(old[0] - high)
                    total = total + factor * old[1]
                    summed = summed + factor * old[2]
                ml = store(r, h, ml, (high, total, summed))
            ml_out[0, r : r + chunk, :] = ml

    if first:
        pl.when(slot == 0)(lambda: compute(True))

        @pl.when((slot > 0) & (mode_ref[slot] > 0))
        def _():
            compute(False)

    else:

        @pl.when(mode_ref[slot] > 0)
        def _():
            compute(False)

    @pl.when((mode_ref[slot] == 0) & ((slot > 0) | (not first)))
    def _():
        for r in range(0, rows, chunk):
            ml = jnp.zeros((chunk, LANES), jnp.float32)
            for h in range(heads):
                old = state_of(r, h)
                if old is None:
                    old = (
                        jnp.full((chunk, 1), very_low, jnp.float32),
                        jnp.zeros((chunk, 1), jnp.float32),
                        jnp.zeros((chunk, head_size), jnp.float32),
                    )
                ml = store(r, h, ml, old)
            ml_out[0, r : r + chunk, :] = ml


def attend_step(mode, starts, queries, pair, gates, state, last, head_size):
    slots, rows, width = queries.shape
    heads = width // head_size
    first = state is None
    chunk = min(rows, 256)
    by_slot = lambda g, *_: (g, 0, 0)
    whole = lambda g, *_: (0, 0)
    in_specs = [
        pl.BlockSpec((1, rows, width), by_slot),
        pl.BlockSpec(pair.shape, whole),
        pl.BlockSpec(gates.shape, whole),
    ]
    state_specs = [pl.BlockSpec((1, rows, width), by_slot), pl.BlockSpec((1, rows, LANES), by_slot)]
    if not first:
        in_specs = in_specs + state_specs
    keys = pair.shape[0]
    return pl.pallas_call(
        functools.partial(attend_kernel, first, last, heads, head_size, chunk),
        out_shape=(
            jax.ShapeDtypeStruct((slots, rows, width), jnp.bfloat16 if last else jnp.float32),
            jax.ShapeDtypeStruct((slots, rows, LANES), jnp.float32),
        ),
        grid_spec=pltpu.PrefetchScalarGridSpec(
            num_scalar_prefetch=2, grid=(slots,), in_specs=in_specs, out_specs=state_specs
        ),
        compiler_params=pltpu.CompilerParams(dimension_semantics=("arbitrary",)),
        cost_estimate=pl.CostEstimate(
            flops=8 * slots * rows * keys * width,
            bytes_accessed=12 * slots * rows * width,
            transcendentals=slots * rows * keys * heads,
        ),
    )(mode, starts, queries, pair, gates, *(() if first else state))


MESH = pl.DeviceIdType.MESH
SUB_ROWS = 128


def layer_kernel(
    tokens_ref, gain_ref, query_weight, key_weight, value_weight, pool_in_weight, gate_ref,
    pool_weight_ref, pool_scale_ref, attention_out, pooling_out, final_gain_ref, out_ref,
    weights, outs, halves, norms, inverse, made, rim, pool_input, extended, pooled, whole, sent, got, row_sums,
    keys, values, queries, results, attended, acc, high,
    w_sem, c_send, c_recv, e_send, e_recv, rim_send, rim_recv,
    z_send, z_recv, x_send, x_recv, y_send, y_recv, r_send, r_recv, o_send, o_recv,
):
    planes, rows, head_size = queries.shape
    width = 2 * halves.shape[2]
    half = width // 2
    inner = made.shape[2]
    groups = pool_weight_ref.shape[0]
    me, core = lax.axis_index("sp"), lax.axis_index("tp")
    devices = lax.axis_size("sp")
    seats = devices // planes
    plane, seat = me // seats, me % seats
    across = seat + 1 - 2 * (seat % 2)
    along = seat + 2 - 4 * (seat // 2)
    far = 3 - seat
    reach = planes - 1

    loads = [
        pltpu.make_async_copy(source, target, w_sem.at[n])
        for n, (source, target) in enumerate(
            [
                (key_weight, weights.at[0]), (value_weight, weights.at[1]), (query_weight, weights.at[2]),
                (pool_in_weight, weights.at[3]), (pooling_out, outs.at[0]), (attention_out, outs.at[1]),
            ]
        )
    ]
    for load in loads:
        load.start()

    def device(p, s):
        return {"sp": p * seats + s}

    sibling = {"tp": 1 - core}

    def block_rows(p, s):
        return pl.ds(pl.multiple_of((p * seats + s) * rows, rows), rows)

    def columns(p):
        return pl.ds(pl.multiple_of(p * head_size, head_size), head_size)

    def key_at(p, s):
        return keys.at[block_rows(p, s), :]

    def value_at(p, s):
        return values.at[block_rows(p, s), pl.ds(0, head_size)]

    def copy(source, target, send, recv, to):
        return pltpu.make_async_remote_copy(
            src_ref=source, dst_ref=target, send_sem=send, recv_sem=recv, device_id=to, device_id_type=MESH
        )

    def arrival(target, recv):
        copy(target, target, z_send.at[0, 0], recv, sibling).wait_recv()

    barrier = pltpu.get_barrier_semaphore()

    def greet(to):
        pl.semaphore_signal(barrier, inc=1, device_id=to, device_id_type=MESH)

    for d in range(1, planes):
        greet(device((plane + d) % planes, seat))
    greet(device(plane, across))
    greet(device(plane, along))
    greet(sibling)
    greet({"sp": (me + 1) % devices})
    greet({"sp": (me + devices - 1) % devices})

    def scale_rows(n, carry):
        at = pl.ds(pl.multiple_of(n * SUB_ROWS, SUB_ROWS), SUB_ROWS)
        widened = tokens_ref[at, :].astype(jnp.float32)
        halves[core, at, :] = (widened * gain_ref[...].astype(jnp.float32)).astype(jnp.bfloat16)
        square = widened * widened
        norms[core, at, :] = functools.reduce(
            jnp.add, [square[:, c : c + LANES] for c in range(0, half, LANES)]
        )
        return carry

    lax.fori_loop(0, rows // SUB_ROWS, scale_rows, 0)
    pl.semaphore_wait(barrier, planes + 4)

    swaps = (
        copy(halves.at[core], halves.at[core], c_send.at[0], c_recv.at[0], sibling),
        copy(norms.at[core], norms.at[core], c_send.at[1], c_recv.at[1], sibling),
    )
    for c in swaps:
        c.start()
    values[:, head_size:] = jnp.ones((values.shape[0], head_size), values.dtype)
    arrival(norms.at[1 - core], c_recv.at[1])
    total = jnp.sum(norms[0] + norms[1], axis=1, keepdims=True)
    inverse[...] = jnp.broadcast_to(lax.rsqrt(total / width + epsilon), inverse.shape)
    arrival(halves.at[1 - core], c_recv.at[0])

    def project(n, factor, store):
        loads[n].wait()

        def one(c, carry):
            at = pl.ds(pl.multiple_of(c * 2 * LANES, 2 * LANES), 2 * LANES)
            r = jnp.dot(halves[0], weights[n, :half, at], preferred_element_type=jnp.float32)
            r = r + jnp.dot(halves[1], weights[n, half:, at], preferred_element_type=jnp.float32)
            f = inverse[...] * factor
            store(at, (r * jnp.concatenate([f, f], axis=1)).astype(jnp.bfloat16))
            return carry

        lax.fori_loop(0, inner // (2 * LANES), one, 0)

    def keep(n):
        def store(at, value):
            made[n, :, at] = value

        return store

    def at_reach(step):
        other = plane + (1 + step // 2) * (1 - 2 * (step % 2))
        return other, (other >= 0) & (other < planes)

    def query_copy(to):
        return copy(
            made.at[2, :, columns(to)], queries.at[plane], z_send.at[2, to], z_recv.at[2, plane], device(to, seat)
        )

    def tensor_copy(n, to):
        target = (key_at, value_at)[n](plane, seat)
        return copy(made.at[n, :, columns(to)], target, z_send.at[n, to], z_recv.at[n, plane], device(to, seat))

    def spread(n, p, own):
        target = (key_at, value_at)[n](p, seat)
        source = made.at[n, :, columns(plane)] if own else target
        return (
            copy(source, target, x_send.at[n, p], x_recv.at[n, p], device(plane, across)),
            copy(source, target, y_send.at[n, p], y_recv.at[n, p], device(plane, along)),
        )

    def relays(p):
        k, v = key_at(p, across), value_at(p, along)
        return (
            copy(k, k, r_send.at[0, p], r_recv.at[0, p], device(plane, along)),
            copy(v, v, r_send.at[1, p], r_recv.at[1, p], device(plane, across)),
        )

    def each(steps, action):
        for step in steps:
            other, valid = at_reach(step)
            pl.when(valid)(functools.partial(action, other))

    def start_all(copies):
        for c in copies:
            c.start()

    def send_pair(to):
        start_all((tensor_copy(0, to), tensor_copy(1, to)))

    project(0, 1.0, keep(0))
    each(range(2), lambda to: tensor_copy(0, to).start())
    start_all(spread(0, plane, True))
    project(1, 1.0, keep(1))
    each(range(2), lambda to: tensor_copy(1, to).start())
    start_all(spread(1, plane, True))
    each(range(2, 2 * reach), send_pair)
    project(2, LOG2E * head_size ** (-0.5), keep(2))
    each(reversed(range(2 * reach)), lambda to: query_copy(to).start())

    keys[block_rows(plane, seat), :] = made[0, :, columns(plane)]
    values[block_rows(plane, seat), :head_size] = made[1, :, columns(plane)]
    queries[plane] = made[2, :, columns(plane)]
    acc[...] = jnp.zeros_like(acc)
    high[...] = jnp.full_like(high, very_low)

    def keep_pool(at, value):
        pool_input[:, at] = value

    project(3, 1.0, keep_pool)
    rim_copy = copy(
        pool_input.at[pl.ds(rows - WINDOW_MAX, WINDOW_MAX), :], rim, rim_send, rim_recv, {"sp": (me + 1) % devices}
    )
    rim_copy.start()

    def forward(p):
        for n in range(2):
            arrival((key_at, value_at)[n](p, seat), z_recv.at[n, p])
            start_all(spread(n, p, False))

    def relay(p):
        to_along, to_across = relays(p)
        arrival(key_at(p, across), x_recv.at[0, p])
        to_along.start()
        arrival(value_at(p, along), y_recv.at[1, p])
        to_across.start()

    def settle(p):
        arrival(value_at(p, across), x_recv.at[1, p])
        arrival(key_at(p, along), y_recv.at[0, p])
        arrival(key_at(p, far), r_recv.at[0, p])
        arrival(value_at(p, far), r_recv.at[1, p])

    span = seats * rows

    def head_gates(here):
        block = gate_ref[:, here]
        mine = lax.broadcasted_iota(jnp.int32, block.shape, 0) == plane
        return jnp.sum(jnp.where(mine, block, 0.0), axis=0, keepdims=True)

    def update(i, p, masked):
        here = pl.ds(pl.multiple_of(p * span, span), span)
        k = keys[here, :]
        v = values[here, :]
        gates = head_gates(here)
        start = head_gates(pl.ds(pl.multiple_of((i * seats + seat) * rows, rows), LANES))[:, :1]
        bias = (start - gates) * LOG2E
        scores = []
        for r in range(0, rows, SUB_ROWS):
            q = queries[i, r : r + SUB_ROWS, :]
            s = lax.dot_general(q, k, (((1,), (1,)), ((), ())), preferred_element_type=jnp.float32) + bias
            if masked:
                row = seat * rows + r + lax.broadcasted_iota(jnp.int32, s.shape, 0)
                s = jnp.where(row >= lax.broadcasted_iota(jnp.int32, s.shape, 1), s, very_low)
            scores.append(s)
        for n, r in enumerate(range(0, rows, SUB_ROWS)):
            s = scores[n]
            at = pl.ds(r, SUB_ROWS)
            old = high[i, at, :]
            new = jnp.maximum(old, jnp.max(s, axis=1, keepdims=True))
            p_ = jnp.exp2(s - new[:, :1]).astype(jnp.bfloat16)
            factor = jnp.exp2(old - new)
            summed = jnp.dot(p_, v, preferred_element_type=jnp.float32)
            acc[i, at, :] = acc[i, at, :] * jnp.concatenate([factor, factor], axis=1) + summed
            high[i, at, :] = new

    def finished(to):
        return copy(
            results.at[to], attended.at[:, columns(plane)], o_send.at[to], o_recv.at[plane], device(to, seat)
        )

    def own_update(p):
        settle(p)

        @pl.when(p < plane)
        def _():
            update(plane, p, False)

        @pl.when(p == plane)
        def _():
            update(plane, p, True)

    def gather(step, carry):
        now, now_valid = at_reach(step)
        before, before_valid = at_reach(step - 1)
        older, older_valid = at_reach(step - 2)
        pl.when((step < 2 * reach) & now_valid)(lambda: forward(now))
        pl.when(step == 0)(lambda: relay(plane))
        pl.when((step > 0) & (step <= 2 * reach) & before_valid)(lambda: relay(before))
        settled = jnp.where(step == 1, plane, older)
        pl.when((step == 1) | ((step > 1) & older_valid))(lambda: own_update(settled))
        return carry

    lax.fori_loop(0, 2 * reach + 2, gather, 0)

    def result_of(i):
        return (acc[i, :, :head_size] / acc[i, :, head_size:]).astype(jnp.bfloat16)

    def serve(step, carry):
        i, valid = at_reach(2 * reach - 1 - step)

        @pl.when(valid)
        def _():
            arrival(queries.at[i], z_recv.at[2, i])

            def earlier(p, carry):
                update(i, p, False)
                return carry

            lax.fori_loop(0, i, earlier, 0)
            update(i, i, True)
            results[i] = result_of(i)
            finished(i).start()

        return carry

    lax.fori_loop(0, 2 * reach, serve, 0)
    attended[:, columns(plane)] = result_of(plane)
    arrival(rim, rim_recv)
    loads[4].wait()

    for g in range(groups):
        at = slice(g * head_size, (g + 1) * head_size)
        window = 2 << (g % 4)
        before = jnp.where(me > 0, rim[:, at].astype(jnp.float32), 0.0)
        current = pool_input[:, at].astype(jnp.float32)
        extended[:WINDOW_MAX, :] = before
        extended[WINDOW_MAX:, :] = current
        depth = 1
        while depth < window:
            total = extended[depth:, :] + extended[: WINDOW_MAX + rows - depth, :]
            extended[depth:, :] = total
            depth = 2 * depth
        location = me * rows + lax.broadcasted_iota(jnp.int32, (rows, head_size), 0)
        count = jnp.minimum(window, location + 1).astype(jnp.float32)
        departure = (extended[WINDOW_MAX:, :] / count - current).astype(jnp.bfloat16)
        mapped = jnp.dot(departure, pool_weight_ref[g], preferred_element_type=jnp.float32)
        pooled[:, at] = (mapped * pool_scale_ref[:, at]).astype(jnp.bfloat16)

    chunks = half // (2 * LANES)

    def out_columns(side, c):
        return pl.ds(pl.multiple_of(side * half + c * 2 * LANES, 2 * LANES), 2 * LANES)

    def chunk_columns(c):
        return pl.ds(pl.multiple_of(c * 2 * LANES, 2 * LANES), 2 * LANES)

    def pool_part(c, carry):
        at = chunk_columns(c)
        whole[:, at] = jnp.dot(pooled[...], outs[0, :, at], preferred_element_type=jnp.float32)
        return carry

    lax.fori_loop(0, 2 * chunks, pool_part, 0)
    loads[5].wait()
    each(range(2 * reach), lambda p: arrival(attended.at[:, columns(p)], o_recv.at[p]))

    def give(c, carry):
        at = out_columns(1 - core, c)
        r = whole[:, at] + jnp.dot(attended[...], outs[1, :, at], preferred_element_type=jnp.float32)
        sent[:, chunk_columns(c)] = r.astype(jnp.bfloat16)
        return carry

    lax.fori_loop(0, chunks, give, 0)
    exchange = copy(sent, got, e_send.at[0], e_recv.at[0], sibling)
    exchange.start()

    def retain(c, carry):
        at = out_columns(core, c)
        whole[:, at] = whole[:, at] + jnp.dot(attended[...], outs[1, :, at], preferred_element_type=jnp.float32)
        return carry

    lax.fori_loop(0, chunks, retain, 0)
    arrival(got, e_recv.at[0])

    def own_half(at_rows):
        return whole[at_rows, pl.ds(pl.multiple_of(core * half, half), half)] + got[at_rows, :].astype(jnp.float32)

    def square_rows(n, carry):
        at = pl.ds(pl.multiple_of(n * SUB_ROWS, SUB_ROWS), SUB_ROWS)
        mixed = own_half(at)
        square = mixed * mixed
        row_sums[core, at, :] = functools.reduce(
            jnp.add, [square[:, c : c + LANES] for c in range(0, half, LANES)]
        )
        return carry

    lax.fori_loop(0, rows // SUB_ROWS, square_rows, 0)
    sums = copy(row_sums.at[core], row_sums.at[core], e_send.at[1], e_recv.at[1], sibling)
    sums.start()
    arrival(row_sums.at[1 - core], e_recv.at[1])

    def finish_rows(n, carry):
        at = pl.ds(pl.multiple_of(n * SUB_ROWS, SUB_ROWS), SUB_ROWS)
        total = jnp.sum(row_sums[0, at, :] + row_sums[1, at, :], axis=1, keepdims=True)
        out_inverse = lax.rsqrt(total / width + epsilon)
        out_ref[at, :] = (own_half(at) * out_inverse * final_gain_ref[...]).astype(jnp.bfloat16)
        return carry

    lax.fori_loop(0, rows // SUB_ROWS, finish_rows, 0)

    def drain(p):
        query_copy(p).wait_send()
        for n in range(2):
            tensor_copy(n, p).wait_send()
            for c in spread(n, p, False):
                c.wait_send()
        for c in relays(p):
            c.wait_send()
        finished(p).wait_send()

    for n in range(2):
        for c in spread(n, plane, True):
            c.wait_send()
    for c in relays(plane):
        c.wait_send()
    each(range(2 * reach), drain)
    for c in swaps + (rim_copy, exchange, sums):
        c.wait_send()


def layer(
    tokens, input_gain, query_weight, key_weight, value_weight, pool_in_weight, log_gates,
    pool_weight, pool_scale, attention_out, pooling_out, final_gain,
):
    rows, half = tokens.shape
    width, inner = query_weight.shape
    planes = log_gates.shape[0]
    head_size = pool_weight.shape[1]
    blocks = lax.axis_size("sp")
    dma = pltpu.SemaphoreType.DMA
    tile = lambda *shape: pltpu.VMEM(shape, jnp.bfloat16)
    wide = lambda *shape: pltpu.VMEM(shape, jnp.float32)
    near = pl.BlockSpec(memory_space=pltpu.VMEM)
    away = pl.BlockSpec(memory_space=pl.ANY)
    pairs = blocks * (blocks + 1) // 2
    return pl.pallas_call(
        layer_kernel,
        out_shape=jax.ShapeDtypeStruct((rows, half), jnp.bfloat16),
        in_specs=[near, near, away, away, away, away, near, near, near, away, away, near],
        out_specs=near,
        scratch_shapes=[
            tile(4, width, inner), tile(2, inner, width), tile(2, rows, half), wide(2, rows, LANES),
            wide(rows, LANES), tile(3, rows, inner), tile(WINDOW_MAX, inner), tile(rows, inner),
            wide(WINDOW_MAX + rows, head_size), tile(rows, inner), wide(rows, width),
            tile(rows, half), tile(rows, half), wide(2, rows, LANES),
            tile(blocks * rows, head_size), tile(blocks * rows, 2 * head_size),
            tile(planes, rows, head_size), tile(planes, rows, head_size), tile(rows, inner),
            wide(planes, rows, 2 * head_size), wide(planes, rows, LANES),
            dma((6,)), dma((2,)), dma((2,)), dma((2,)), dma((2,)), dma, dma,
            dma((3, planes)), dma((3, planes)),
            dma((2, planes)), dma((2, planes)),
            dma((2, planes)), dma((2, planes)),
            dma((2, planes)), dma((2, planes)),
            dma((planes,)), dma((planes,)),
        ],
        compiler_params=pltpu.CompilerParams(
            collective_id=0, has_side_effects=True, vmem_limit_bytes=56 * 2**20
        ),
        cost_estimate=pl.CostEstimate(
            flops=4 * pairs * rows * rows * head_size + 12 * rows * width * inner,
            bytes_accessed=12 * width * inner,
            transcendentals=pairs * rows * rows,
        ),
    )(
        tokens, input_gain.reshape(1, -1), query_weight, key_weight, value_weight, pool_in_weight, log_gates,
        pool_weight, pool_scale.reshape(1, -1), attention_out, pooling_out, final_gain.reshape(1, -1),
    )


def ring_attend(query, keys, values, log_gates):
    tok_rows = query.shape[0]
    heads = log_gates.shape[0]
    head_size = query.shape[1] // heads
    devices = lax.axis_size("sp")
    side = 1
    while (2 * side) ** 2 <= devices and devices % (2 * side) == 0:
        side = 2 * side
    planes = devices // side
    sequence_index = lax.axis_index("sp")
    plane = sequence_index // side
    seat = sequence_index % side
    pair = jnp.concatenate([keys, values], axis=1)
    pairs = [pair]
    for _ in range(1, planes):
        pairs.append(passed_along(pairs[-1], "sp", side))
    queries = jnp.stack([query] + [swapped(query, "sp", g) for g in range(1, side)])
    seats = seat ^ jnp.arange(side, dtype=jnp.int32)
    starts = jnp.stack(
        [
            lax.dynamic_slice_in_dim(log_gates, (plane * side + (seat ^ g)) * tok_rows, 1, 1)[:, 0]
            for g in range(side)
        ]
    ).reshape(-1)
    state = None
    for k in range(planes):
        source = jnp.maximum(sequence_index - k * side, seat)
        gates = lax.dynamic_slice_in_dim(log_gates, source * tok_rows, tok_rows, 1)
        if k == 0:
            mode = (seats > seat).astype(jnp.int32)
        else:
            mode = jnp.full((side,), plane >= k, jnp.int32)
        state = attend_step(
            mode, starts, queries, pairs[k], gates, state, k == planes - 1, head_size
        )
    partial, level = state
    level = level[:, :, :heads]
    shares = [partial[0]] + [swapped(partial[g], "sp", g) for g in range(1, side)]
    tall = jnp.transpose(level, (0, 2, 1))
    levels = jnp.stack([tall[0]] + [swapped(tall[g], "sp", g) for g in range(1, side)])
    portion = jnp.exp2(levels - jnp.max(levels, axis=0, keepdims=True))
    portion = portion / jnp.sum(portion, axis=0, keepdims=True)
    portion = jnp.transpose(portion, (0, 2, 1))
    attended = 0.0
    for g in range(side):
        attended = attended + shares[g].astype(jnp.float32) * jnp.repeat(portion[g], head_size, axis=1)
    return attended.astype(jnp.bfloat16)


def gathered(block, axis):
    if lax.axis_size(axis) != 2:
        return lax.all_gather(block, axis, axis=1, tiled=True)
    other = swapped(block, axis, 1)
    lower = lax.axis_index(axis) == 0
    return jnp.concatenate([jnp.where(lower, block, other), jnp.where(lower, other, block)], axis=1)


def body(
    tokens,
    input_gain,
    query_weight,
    key_weight,
    value_weight,
    pool_in_weight,
    log_gates,
    pool_weight,
    pool_scale,
    attention_out,
    pooling_out,
    final_gain,
):
    tok_rows = tokens.shape[0]
    width = query_weight.shape[0]
    groups = pool_weight.shape[0]
    head_size = pool_weight.shape[1]
    heads = log_gates.shape[0]
    attention_width = query_weight.shape[1]
    pool_width = pool_in_weight.shape[1]
    devices = lax.axis_size("sp")
    shards = lax.axis_size("tp")
    sequence_index = lax.axis_index("sp")
    first_row = sequence_index * tok_rows
    if shards == 2 and groups % 4 == 0 and heads > 1 and devices == 4 * heads and attention_width == pool_width:
        return layer(
            tokens, input_gain, query_weight, key_weight, value_weight, pool_in_weight, log_gates,
            pool_weight, pool_scale, attention_out, pooling_out, final_gain,
        )

    part = gathered(tokens, "tp")
    gain_part = gathered(input_gain.reshape(1, -1), "tp")
    widened = part.astype(jnp.float32)
    scaled = (widened * gain_part.astype(jnp.float32)).astype(jnp.bfloat16)

    def product(weight):
        return jnp.dot(scaled, weight, preferred_element_type=jnp.float32)

    inverse = lax.rsqrt(jnp.sum(widened * widened, axis=1) / width + epsilon)[:, None]
    keys = (product(key_weight) * inverse).astype(jnp.bfloat16)
    values = (product(value_weight) * inverse).astype(jnp.bfloat16)
    query = (product(query_weight) * (inverse * (LOG2E * head_size ** (-0.5)))).astype(jnp.bfloat16)
    pool_input = (product(pool_in_weight) * inverse).astype(jnp.bfloat16)
    rim = passed_along(pool_input[tok_rows - (WINDOW_MAX - 1) :], "sp", 1)

    attended = ring_attend(query, keys, values, log_gates)

    extended = jnp.concatenate([rim, pool_input], axis=0).astype(jnp.float32)
    column = jnp.arange(pool_width, dtype=jnp.int32)
    group_number = lax.axis_index("tp") * groups + column // head_size
    window = jnp.left_shift(jnp.full((pool_width,), 2, jnp.int32), group_number % 4)
    sums = extended
    span = 1
    chosen = jnp.zeros((tok_rows, pool_width), jnp.float32)
    for _ in range(4):
        sums = sums[span:] + sums[:-span]
        span = span * 2
        offset_rows = WINDOW_MAX - span
        chosen = jnp.where(window[None, :] == span, sums[offset_rows : offset_rows + tok_rows], chosen)
    element_locations = first_row + jnp.arange(tok_rows, dtype=jnp.int32)
    counts = jnp.minimum(window[None, :], element_locations[:, None] + 1).astype(jnp.float32)
    departure = (chosen / counts - pool_input.astype(jnp.float32)).astype(jnp.bfloat16)
    mapped = jnp.concatenate(
        [
            jnp.dot(
                departure[:, g * head_size : (g + 1) * head_size],
                pool_weight[g],
                preferred_element_type=jnp.float32,
            )
            for g in range(groups)
        ],
        axis=1,
    )
    pooled = (mapped * pool_scale).astype(jnp.bfloat16)
    pooled_part = jnp.dot(pooled, pooling_out, preferred_element_type=jnp.float32)
    whole = jnp.dot(attended, attention_out, preferred_element_type=jnp.float32) + pooled_part
    if shards == 2:
        half = width // 2
        lower = lax.axis_index("tp") == 0
        sent = jnp.where(lower, whole[:, half:], whole[:, :half]).astype(jnp.bfloat16)
        kept = jnp.where(lower, whole[:, :half], whole[:, half:])
        mixed = kept + swapped(sent, "tp", 1).astype(jnp.float32)
        squares = jnp.sum(mixed * mixed, axis=1)
        squares = squares + swapped(squares, "tp", 1)
    else:
        mixed = lax.psum_scatter(
            whole.astype(jnp.bfloat16), "tp", scatter_dimension=1, tiled=True
        ).astype(jnp.float32)
        squares = lax.psum(jnp.sum(mixed * mixed, axis=1), "tp")
    out_inverse = lax.rsqrt(squares / width + epsilon)
    return (mixed * out_inverse[:, None] * final_gain[None, :]).astype(jnp.bfloat16)


def solution(mesh):
    return jax.shard_map(
        body,
        mesh=mesh,
        in_specs=(
            P("sp", "tp"),
            P("tp"),
            P(None, "tp"),
            P(None, "tp"),
            P(None, "tp"),
            P(None, "tp"),
            P("tp", None),
            P("tp", None, None),
            P("tp"),
            P("tp", None),
            P("tp", None),
            P("tp"),
        ),
        out_specs=P("sp", "tp"),
        check_vma=False,
    )
```

```python
import functools

import jax
import jax.numpy as jnp
from jax import lax
from jax.experimental import pallas as pl
from jax.experimental.pallas import tpu as pltpu
from jax.sharding import PartitionSpec as P


WINDOW_MAX = 16
LANES = 128
LOG2E = 1.4426950408889634

very_low = -1e30
epsilon = 1e-06


def passed_along(block, axis, distance):
    devices = range(lax.axis_size(axis))
    route = [(i - distance, i) for i in devices if i - distance in devices]
    return lax.ppermute(block, axis, route)


def swapped(block, axis, offset):
    return lax.ppermute(block, axis, [(i, i ^ offset) for i in range(lax.axis_size(axis))])


def attend_kernel(first, last, heads, head_size, chunk, mode_ref, start_ref, *refs):
    if first:
        q_ref, kv_ref, gate_ref, acc_out, ml_out = refs
    else:
        q_ref, kv_ref, gate_ref, acc_in, ml_in, acc_out, ml_out = refs
    slot = pl.program_id(0)
    rows = q_ref.shape[1]
    keys = kv_ref.shape[0]
    width = heads * head_size
    lane = lax.broadcasted_iota(jnp.int32, (chunk, LANES), 1)

    def state_of(r, h):
        if first:
            return None
        ml = ml_in[0, r : r + chunk, :]
        columns = slice(h * head_size, (h + 1) * head_size)
        return (ml[:, h : h + 1], ml[:, heads + h : heads + h + 1], acc_in[0, r : r + chunk, columns])

    def store(r, h, ml, state):
        columns = slice(h * head_size, (h + 1) * head_size)
        high, total, summed = state
        if last:
            safe = jnp.where(total > 0.0, total, 1.0)
            acc_out[0, r : r + chunk, columns] = (summed / safe).astype(acc_out.dtype)
            level = jnp.where(total > 0.0, high + jnp.log2(safe), very_low)
            return jnp.where(lane == h, level, ml)
        acc_out[0, r : r + chunk, columns] = summed
        return jnp.where(lane == h, high, jnp.where(lane == heads + h, total, ml))

    def compute(diagonal):
        for r in range(0, rows, chunk):
            ml = jnp.zeros((chunk, LANES), jnp.float32)
            span = min(r + chunk, keys) if diagonal else keys
            for h in range(heads):
                columns = slice(h * head_size, (h + 1) * head_size)
                q = q_ref[0, r : r + chunk, columns]
                k = kv_ref[:span, columns]
                v = kv_ref[:span, width + h * head_size : width + (h + 1) * head_size]
                bias = (start_ref[slot * heads + h] - gate_ref[h : h + 1, :span]) * LOG2E
                s = lax.dot_general(q, k, (((1,), (1,)), ((), ())), preferred_element_type=jnp.float32)
                s = s + bias
                if diagonal:
                    row = r + lax.broadcasted_iota(jnp.int32, s.shape, 0)
                    s = jnp.where(row >= lax.broadcasted_iota(jnp.int32, s.shape, 1), s, very_low)
                old = state_of(r, h)
                high = jnp.max(s, axis=1, keepdims=True)
                if old is not None:
                    high = jnp.maximum(high, old[0])
                p = jnp.exp2(s - high)
                total = jnp.sum(p, axis=1, keepdims=True)
                summed = jnp.dot(p.astype(jnp.bfloat16), v, preferred_element_type=jnp.float32)
                if old is not None:
                    factor = jnp.exp2(old[0] - high)
                    total = total + factor * old[1]
                    summed = summed + factor * old[2]
                ml = store(r, h, ml, (high, total, summed))
            ml_out[0, r : r + chunk, :] = ml

    if first:
        pl.when(slot == 0)(lambda: compute(True))

        @pl.when((slot > 0) & (mode_ref[slot] > 0))
        def _():
            compute(False)

    else:

        @pl.when(mode_ref[slot] > 0)
        def _():
            compute(False)

    @pl.when((mode_ref[slot] == 0) & ((slot > 0) | (not first)))
    def _():
        for r in range(0, rows, chunk):
            ml = jnp.zeros((chunk, LANES), jnp.float32)
            for h in range(heads):
                old = state_of(r, h)
                if old is None:
                    old = (
                        jnp.full((chunk, 1), very_low, jnp.float32),
                        jnp.zeros((chunk, 1), jnp.float32),
                        jnp.zeros((chunk, head_size), jnp.float32),
                    )
                ml = store(r, h, ml, old)
            ml_out[0, r : r + chunk, :] = ml


def attend_step(mode, starts, queries, pair, gates, state, last, head_size):
    slots, rows, width = queries.shape
    heads = width // head_size
    first = state is None
    chunk = min(rows, 256)
    by_slot = lambda g, *_: (g, 0, 0)
    whole = lambda g, *_: (0, 0)
    in_specs = [
        pl.BlockSpec((1, rows, width), by_slot),
        pl.BlockSpec(pair.shape, whole),
        pl.BlockSpec(gates.shape, whole),
    ]
    state_specs = [pl.BlockSpec((1, rows, width), by_slot), pl.BlockSpec((1, rows, LANES), by_slot)]
    if not first:
        in_specs = in_specs + state_specs
    keys = pair.shape[0]
    return pl.pallas_call(
        functools.partial(attend_kernel, first, last, heads, head_size, chunk),
        out_shape=(
            jax.ShapeDtypeStruct((slots, rows, width), jnp.bfloat16 if last else jnp.float32),
            jax.ShapeDtypeStruct((slots, rows, LANES), jnp.float32),
        ),
        grid_spec=pltpu.PrefetchScalarGridSpec(
            num_scalar_prefetch=2, grid=(slots,), in_specs=in_specs, out_specs=state_specs
        ),
        compiler_params=pltpu.CompilerParams(dimension_semantics=("arbitrary",)),
        cost_estimate=pl.CostEstimate(
            flops=8 * slots * rows * keys * width,
            bytes_accessed=12 * slots * rows * width,
            transcendentals=slots * rows * keys * heads,
        ),
    )(mode, starts, queries, pair, gates, *(() if first else state))


MESH = pl.DeviceIdType.MESH
SUB_ROWS = 128


def layer_kernel(
    tokens_ref, gain_ref, query_weight, key_weight, value_weight, pool_in_weight, gate_ref,
    pool_weight_ref, pool_scale_ref, attention_out, pooling_out, final_gain_ref, out_ref,
    weights, outs, halves, norms, inverse, made, parts, rim, pool_input, extended, pooled, whole, sent, got, row_sums,
    pairs, other_gates, gate_row, queries, results, attended, acc, high,
    w_sem, c_send, c_recv, e_send, e_recv, rim_send, rim_recv,
    q_send, q_recv, t_send, t_recv, y_send, y_recv, s_send, s_recv, f_send, f_recv, o_send, o_recv,
):
    planes, rows, head_size = queries.shape
    width = 2 * halves.shape[2]
    half = width // 2
    inner = made.shape[2]
    groups = pool_weight_ref.shape[0]
    me, core = lax.axis_index("sp"), lax.axis_index("tp")
    devices = lax.axis_size("sp")
    seats = devices // planes
    plane, seat = me // seats, me % seats
    line, side = seat // 2, seat % 2
    maker = plane % 2
    reach = planes - 1
    span = seats * rows

    loads = [
        pltpu.make_async_copy(source, target, w_sem.at[n])
        for n, (source, target) in enumerate(
            [
                (key_weight, weights.at[0]), (value_weight, weights.at[1]), (query_weight, weights.at[2]),
                (pool_in_weight, weights.at[3]), (pooling_out, outs.at[0]), (attention_out, outs.at[1]),
            ]
        )
    ]
    for load in loads:
        load.start()

    def device(p, y, x, c):
        return {"sp": p * seats + 2 * y + x, "tp": c}

    sibling = {"tp": 1 - core}

    def columns(l):
        return pl.ds(pl.multiple_of(l * head_size, head_size), head_size)

    def kept(p, x):
        return 2 * (p // 2) + x

    own = kept(plane, side)

    def away(p, x, c):
        return (p != plane) | (x != side) | (c != core)

    def block_rows(p, y, x):
        return pl.ds(pl.multiple_of((p * seats + 2 * y + x) * rows, rows), rows)

    def block(t, p, y, x):
        return pairs.at[t, block_rows(p, y, x), pl.ds(0, head_size)]

    def copy(source, target, send, recv, to):
        return pltpu.make_async_remote_copy(
            src_ref=source, dst_ref=target, send_sem=send, recv_sem=recv, device_id=to, device_id_type=MESH
        )

    def arrival(target, recv):
        copy(target, target, q_send.at[0], recv, sibling).wait_recv()

    barrier = pltpu.get_barrier_semaphore()

    def greet(to):
        pl.semaphore_signal(barrier, inc=1, device_id=to, device_id_type=MESH)

    for p in range(planes):
        for x in range(2):
            for c in range(2):
                pl.when(away(p, x, c))(functools.partial(greet, device(p, line, x, c)))
    greet(device(plane, 1 - line, side, core))
    greet({"sp": (me + 1) % devices})
    greet({"sp": (me + devices - 1) % devices})

    def scale_rows(n, carry):
        at = pl.ds(pl.multiple_of(n * SUB_ROWS, SUB_ROWS), SUB_ROWS)
        widened = tokens_ref[at, :].astype(jnp.float32)
        halves[core, at, :] = (widened * gain_ref[...].astype(jnp.float32)).astype(jnp.bfloat16)
        square = widened * widened
        norms[core, at, :] = functools.reduce(
            jnp.add, [square[:, c : c + LANES] for c in range(0, half, LANES)]
        )
        return carry

    lax.fori_loop(0, rows // SUB_ROWS, scale_rows, 0)
    pl.semaphore_wait(barrier, 4 * planes + 2)

    swaps = (
        copy(halves.at[core], halves.at[core], c_send.at[0], c_recv.at[0], sibling),
        copy(norms.at[core], norms.at[core], c_send.at[1], c_recv.at[1], sibling),
        copy(gate_ref, other_gates, c_send.at[2], c_recv.at[2], sibling),
    )
    for c in swaps:
        c.start()

    def project(use):
        def one(c, carry):
            use(pl.ds(pl.multiple_of(c * 2 * LANES, 2 * LANES), 2 * LANES))
            return carry

        lax.fori_loop(0, inner // (2 * LANES), one, 0)

    def product(h, n, at):
        here = pl.ds(pl.multiple_of(h * half, half), half)
        return jnp.dot(halves[h], weights[n, here, at], preferred_element_type=jnp.float32)

    for n in range(3):
        loads[n].wait()

        def begin(at):
            parts[n, :, at] = product(core, n, at)

        project(begin)
    pairs[1, :, head_size:] = jnp.ones((pairs.shape[1], head_size), pairs.dtype)
    arrival(norms.at[1 - core], c_recv.at[1])
    total = jnp.sum(norms[0] + norms[1], axis=1, keepdims=True)
    inverse[...] = jnp.broadcast_to(lax.rsqrt(total / width + epsilon), inverse.shape)
    arrival(halves.at[1 - core], c_recv.at[0])

    def scaled_by(factor, r):
        f = inverse[...] * factor
        return (r * jnp.concatenate([f, f], axis=1)).astype(jnp.bfloat16)

    def complete(n, factor):
        def use(at):
            made[n, :, at] = scaled_by(factor, parts[n, :, at] + product(1 - core, n, at))

        project(use)

    def query_copy(p, x):
        l = kept(p, x)
        return copy(
            made.at[2, :, columns(l)], queries.at[plane], q_send.at[l], q_recv.at[plane], device(p, line, x, side)
        )

    def tensor_copy(t, p, x):
        l = kept(p, x)
        return copy(
            made.at[t, :, columns(l)], block(t, plane, line, side),
            t_send.at[t, l], t_recv.at[2 * plane + side], device(p, line, x, t),
        )

    served = [2 * n + core for n in range(planes // 2)]

    def send_tensor(t, p, wanted):
        for x in (side, 1 - side):
            pl.when(wanted & away(p, x, t))(lambda: tensor_copy(t, p, x).start())

    def send_query(p, wanted):
        for x in (side, 1 - side):
            pl.when(wanted & away(p, x, side))(lambda: query_copy(p, x).start())

    def onward(p, x, source):
        n = 2 * p + x
        target = block(core, p, line, x)
        return (
            copy(source, target, y_send.at[n], y_recv.at[n], device(plane, 1 - line, side, core)),
            copy(source, target, s_send.at[n], s_recv.at[n], sibling),
        )

    def start_all(copies):
        for c in copies:
            c.start()

    mine = maker == core
    complete(0, 1.0)
    for p in served:
        send_tensor(0, p, p == plane)
    send_tensor(0, served[0], served[0] > plane)
    complete(1, 1.0)
    for p in served:
        send_tensor(1, p, p == plane)
    pl.when(mine)(lambda: start_all(onward(plane, side, made.at[core, :, columns(own)])))
    send_tensor(1, served[0], served[0] > plane)
    for p in served[1:]:
        send_tensor(0, p, p > plane)
        send_tensor(1, p, p > plane)
    complete(2, LOG2E * head_size ** (-0.5))
    for p in served:
        send_query(p, p <= plane)
    for p in reversed(served):
        send_tensor(0, p, p < plane)
        send_tensor(1, p, p < plane)
    for p in reversed(served):
        send_query(p, p > plane)

    @pl.when(mine)
    def _():
        pairs[core, block_rows(plane, line, side), :head_size] = made[core, :, columns(own)]

    @pl.when(mine & (side == core))
    def _():
        queries[plane] = made[2, :, columns(own)]

    arrival(other_gates, c_recv.at[2])
    gates = jnp.where(mine, gate_ref[...], other_gates[...])
    chosen = lax.broadcasted_iota(jnp.int32, gates.shape, 0) == own
    gate_row[...] = jnp.sum(jnp.where(chosen, gates, 0.0), axis=0, keepdims=True)
    acc[...] = jnp.zeros_like(acc)
    high[...] = jnp.full_like(high, very_low)

    loads[3].wait()

    def pool_product(at):
        pool_input[:, at] = scaled_by(1.0, product(0, 3, at) + product(1, 3, at))

    project(pool_product)
    rim_copy = copy(
        pool_input.at[pl.ds(rows - WINDOW_MAX, WINDOW_MAX), :], rim, rim_send, rim_recv, {"sp": (me + 1) % devices}
    )
    rim_copy.start()

    def forward(p):
        for x in (side, 1 - side):
            held = block(core, p, line, x)

            @pl.when(jnp.logical_not(mine & (p == plane) & (x == side)))
            def _():
                arrival(held, t_recv.at[2 * p + x])
                start_all(onward(p, x, held))

    def beside(p, x):
        n = 2 * p + x
        held = block(core, p, 1 - line, x)
        return copy(held, held, f_send.at[n], f_recv.at[n], sibling)

    def relay(p):
        for x in (side, 1 - side):
            arrival(block(core, p, 1 - line, x), y_recv.at[2 * p + x])
            beside(p, x).start()

    def settle(p):
        for x in range(2):
            arrival(block(1 - core, p, line, x), s_recv.at[2 * p + x])
            arrival(block(1 - core, p, 1 - line, x), f_recv.at[2 * p + x])

    place = 2 * line + core

    def update(i, p, masked):
        here = pl.ds(pl.multiple_of(p * span, span), span)
        k = pairs[0, here, :head_size]
        v = pairs[1, here, :]
        gates = gate_row[:, here]
        start = gate_row[:, pl.ds(pl.multiple_of((i * seats + place) * rows, rows), LANES)][:, :1]
        bias = (start - gates) * LOG2E
        scores = []
        for r in range(0, rows, SUB_ROWS):
            q = queries[i, r : r + SUB_ROWS, :]
            s = lax.dot_general(q, k, (((1,), (1,)), ((), ())), preferred_element_type=jnp.float32) + bias
            if masked:
                row = place * rows + r + lax.broadcasted_iota(jnp.int32, s.shape, 0)
                s = jnp.where(row >= lax.broadcasted_iota(jnp.int32, s.shape, 1), s, very_low)
            scores.append(s)
        for n, r in enumerate(range(0, rows, SUB_ROWS)):
            s = scores[n]
            at = pl.ds(r, SUB_ROWS)
            old = high[i, at, :]
            new = jnp.maximum(old, jnp.max(s, axis=1, keepdims=True))
            p_ = jnp.exp2(s - new[:, :1]).astype(jnp.bfloat16)
            factor = jnp.exp2(old - new)
            summed = jnp.dot(p_, v, preferred_element_type=jnp.float32)
            acc[i, at, :] = acc[i, at, :] * jnp.concatenate([factor, factor], axis=1) + summed
            high[i, at, :] = new

    def finished(i):
        return copy(
            results.at[i], attended.at[:, columns(own)], o_send.at[i], o_recv.at[own], device(i, line, core, maker)
        )

    def query_arrival(i):
        pl.when(away(i, core, maker))(lambda: arrival(queries.at[i], q_recv.at[i]))

    def result_of(i):
        return (acc[i, :, :head_size] / acc[i, :, head_size:]).astype(jnp.bfloat16)

    def give_back(i):
        @pl.when(away(i, core, maker))
        def _():
            results[i] = result_of(i)
            finished(i).start()

        @pl.when(jnp.logical_not(away(i, core, maker)))
        def _():
            attended[:, columns(own)] = result_of(i)

    def source(n):
        return jnp.where(n <= plane, plane - n, n)

    def step(n, carry):
        p = source(n)
        late = (n == 0) & (plane == 0)
        more = n < reach
        relay(p)
        pl.when(more & jnp.logical_not(late))(lambda: forward(source(n + 1)))
        settle(p)

        def one(i, carry):
            pl.when(n == 0)(lambda: query_arrival(i))
            pl.when(i > p)(lambda: update(i, p, False))
            pl.when(i == p)(lambda: update(i, p, True))
            pl.when((i == p) & (i > plane))(lambda: give_back(i))
            return carry

        lax.fori_loop(jnp.where(p > plane, p, plane), planes, one, 0)
        pl.when(late)(lambda: forward(source(n + 1)))
        return carry

    forward(plane)
    lax.fori_loop(0, planes, step, 0)

    def serve(i, carry):
        query_arrival(i)

        def earlier(p, carry):
            update(i, p, False)
            return carry

        lax.fori_loop(0, i, earlier, 0)
        update(i, i, True)
        give_back(i)
        return carry

    lax.fori_loop(0, plane, serve, 0)
    give_back(plane)
    arrival(rim, rim_recv)
    loads[4].wait()

    for g in range(groups):
        at = slice(g * head_size, (g + 1) * head_size)
        window = 2 << (g % 4)
        before = jnp.where(me > 0, rim[:, at].astype(jnp.float32), 0.0)
        current = pool_input[:, at].astype(jnp.float32)
        extended[:WINDOW_MAX, :] = before
        extended[WINDOW_MAX:, :] = current
        depth = 1
        while depth < window:
            total = extended[depth:, :] + extended[: WINDOW_MAX + rows - depth, :]
            extended[depth:, :] = total
            depth = 2 * depth
        location = me * rows + lax.broadcasted_iota(jnp.int32, (rows, head_size), 0)
        count = jnp.minimum(window, location + 1).astype(jnp.float32)
        departure = (extended[WINDOW_MAX:, :] / count - current).astype(jnp.bfloat16)
        mapped = jnp.dot(departure, pool_weight_ref[g], preferred_element_type=jnp.float32)
        pooled[:, at] = (mapped * pool_scale_ref[:, at]).astype(jnp.bfloat16)

    chunks = half // (2 * LANES)

    def out_columns(side, c):
        return pl.ds(pl.multiple_of(side * half + c * 2 * LANES, 2 * LANES), 2 * LANES)

    def chunk_columns(c):
        return pl.ds(pl.multiple_of(c * 2 * LANES, 2 * LANES), 2 * LANES)

    def pool_part(c, carry):
        at = chunk_columns(c)
        whole[:, at] = jnp.dot(pooled[...], outs[0, :, at], preferred_element_type=jnp.float32)
        return carry

    lax.fori_loop(0, 2 * chunks, pool_part, 0)
    loads[5].wait()
    for p in served:
        for x in range(2):
            l = kept(p, x)
            pl.when(away(p, x, side))(lambda: arrival(attended.at[:, columns(l)], o_recv.at[l]))

    def give(c, carry):
        at = out_columns(1 - core, c)
        r = whole[:, at] + jnp.dot(attended[...], outs[1, :, at], preferred_element_type=jnp.float32)
        sent[:, chunk_columns(c)] = r.astype(jnp.bfloat16)
        return carry

    lax.fori_loop(0, chunks, give, 0)
    exchange = copy(sent, got, e_send.at[0], e_recv.at[0], sibling)
    exchange.start()

    def retain(c, carry):
        at = out_columns(core, c)
        whole[:, at] = whole[:, at] + jnp.dot(attended[...], outs[1, :, at], preferred_element_type=jnp.float32)
        return carry

    lax.fori_loop(0, chunks, retain, 0)
    arrival(got, e_recv.at[0])

    def own_half(at_rows):
        return whole[at_rows, pl.ds(pl.multiple_of(core * half, half), half)] + got[at_rows, :].astype(jnp.float32)

    def square_rows(n, carry):
        at = pl.ds(pl.multiple_of(n * SUB_ROWS, SUB_ROWS), SUB_ROWS)
        mixed = own_half(at)
        square = mixed * mixed
        row_sums[core, at, :] = functools.reduce(
            jnp.add, [square[:, c : c + LANES] for c in range(0, half, LANES)]
        )
        return carry

    lax.fori_loop(0, rows // SUB_ROWS, square_rows, 0)
    sums = copy(row_sums.at[core], row_sums.at[core], e_send.at[1], e_recv.at[1], sibling)
    sums.start()
    arrival(row_sums.at[1 - core], e_recv.at[1])

    def finish_rows(n, carry):
        at = pl.ds(pl.multiple_of(n * SUB_ROWS, SUB_ROWS), SUB_ROWS)
        total = jnp.sum(row_sums[0, at, :] + row_sums[1, at, :], axis=1, keepdims=True)
        out_inverse = lax.rsqrt(total / width + epsilon)
        out_ref[at, :] = (own_half(at) * out_inverse * final_gain_ref[...]).astype(jnp.bfloat16)
        return carry

    lax.fori_loop(0, rows // SUB_ROWS, finish_rows, 0)

    for p in served:
        for x in range(2):
            pl.when(away(p, x, side))(lambda: query_copy(p, x).wait_send())
            for t in range(2):
                pl.when(away(p, x, t))(lambda: tensor_copy(t, p, x).wait_send())
    for p in range(planes):
        for x in range(2):
            for c in onward(p, x, block(core, p, line, x)):
                c.wait_send()
            beside(p, x).wait_send()
        pl.when(away(p, core, maker))(lambda: finished(p).wait_send())
    for c in swaps + (rim_copy, exchange, sums):
        c.wait_send()


def layer(
    tokens, input_gain, query_weight, key_weight, value_weight, pool_in_weight, log_gates,
    pool_weight, pool_scale, attention_out, pooling_out, final_gain,
):
    rows, half = tokens.shape
    width, inner = query_weight.shape
    planes = log_gates.shape[0]
    head_size = pool_weight.shape[1]
    blocks = lax.axis_size("sp")
    dma = pltpu.SemaphoreType.DMA
    tile = lambda *shape: pltpu.VMEM(shape, jnp.bfloat16)
    wide = lambda *shape: pltpu.VMEM(shape, jnp.float32)
    near = pl.BlockSpec(memory_space=pltpu.VMEM)
    away = pl.BlockSpec(memory_space=pl.ANY)
    pairs = blocks * (blocks + 1) // 2
    return pl.pallas_call(
        layer_kernel,
        out_shape=jax.ShapeDtypeStruct((rows, half), jnp.bfloat16),
        in_specs=[near, near, away, away, away, away, near, near, near, away, away, near],
        out_specs=near,
        scratch_shapes=[
            tile(4, width, inner), tile(2, inner, width), tile(2, rows, half), wide(2, rows, LANES),
            wide(rows, LANES), tile(3, rows, inner), wide(3, rows, inner), tile(WINDOW_MAX, inner), tile(rows, inner),
            wide(WINDOW_MAX + rows, head_size), tile(rows, inner), wide(rows, width),
            tile(rows, half), tile(rows, half), wide(2, rows, LANES),
            tile(2, blocks * rows, 2 * head_size), wide(*log_gates.shape), wide(1, blocks * rows),
            tile(planes, rows, head_size), tile(planes, rows, head_size), tile(rows, inner),
            wide(planes, rows, 2 * head_size), wide(planes, rows, LANES),
            dma((6,)), dma((3,)), dma((3,)), dma((2,)), dma((2,)), dma, dma,
            dma((planes,)), dma((planes,)),
            dma((2, planes)), dma((2 * planes,)),
            dma((2 * planes,)), dma((2 * planes,)),
            dma((2 * planes,)), dma((2 * planes,)),
            dma((2 * planes,)), dma((2 * planes,)),
            dma((planes,)), dma((planes,)),
        ],
        compiler_params=pltpu.CompilerParams(
            collective_id=0, has_side_effects=True, vmem_limit_bytes=56 * 2**20
        ),
        cost_estimate=pl.CostEstimate(
            flops=4 * pairs * rows * rows * head_size + 12 * rows * width * inner,
            bytes_accessed=12 * width * inner,
            transcendentals=pairs * rows * rows,
        ),
    )(
        tokens, input_gain.reshape(1, -1), query_weight, key_weight, value_weight, pool_in_weight, log_gates,
        pool_weight, pool_scale.reshape(1, -1), attention_out, pooling_out, final_gain.reshape(1, -1),
    )


def ring_attend(query, keys, values, log_gates):
    tok_rows = query.shape[0]
    heads = log_gates.shape[0]
    head_size = query.shape[1] // heads
    devices = lax.axis_size("sp")
    side = 1
    while (2 * side) ** 2 <= devices and devices % (2 * side) == 0:
        side = 2 * side
    planes = devices // side
    sequence_index = lax.axis_index("sp")
    plane = sequence_index // side
    seat = sequence_index % side
    pair = jnp.concatenate([keys, values], axis=1)
    pairs = [pair]
    for _ in range(1, planes):
        pairs.append(passed_along(pairs[-1], "sp", side))
    queries = jnp.stack([query] + [swapped(query, "sp", g) for g in range(1, side)])
    seats = seat ^ jnp.arange(side, dtype=jnp.int32)
    starts = jnp.stack(
        [
            lax.dynamic_slice_in_dim(log_gates, (plane * side + (seat ^ g)) * tok_rows, 1, 1)[:, 0]
            for g in range(side)
        ]
    ).reshape(-1)
    state = None
    for k in range(planes):
        source = jnp.maximum(sequence_index - k * side, seat)
        gates = lax.dynamic_slice_in_dim(log_gates, source * tok_rows, tok_rows, 1)
        if k == 0:
            mode = (seats > seat).astype(jnp.int32)
        else:
            mode = jnp.full((side,), plane >= k, jnp.int32)
        state = attend_step(
            mode, starts, queries, pairs[k], gates, state, k == planes - 1, head_size
        )
    partial, level = state
    level = level[:, :, :heads]
    shares = [partial[0]] + [swapped(partial[g], "sp", g) for g in range(1, side)]
    tall = jnp.transpose(level, (0, 2, 1))
    levels = jnp.stack([tall[0]] + [swapped(tall[g], "sp", g) for g in range(1, side)])
    portion = jnp.exp2(levels - jnp.max(levels, axis=0, keepdims=True))
    portion = portion / jnp.sum(portion, axis=0, keepdims=True)
    portion = jnp.transpose(portion, (0, 2, 1))
    attended = 0.0
    for g in range(side):
        attended = attended + shares[g].astype(jnp.float32) * jnp.repeat(portion[g], head_size, axis=1)
    return attended.astype(jnp.bfloat16)


def gathered(block, axis):
    if lax.axis_size(axis) != 2:
        return lax.all_gather(block, axis, axis=1, tiled=True)
    other = swapped(block, axis, 1)
    lower = lax.axis_index(axis) == 0
    return jnp.concatenate([jnp.where(lower, block, other), jnp.where(lower, other, block)], axis=1)


def body(
    tokens,
    input_gain,
    query_weight,
    key_weight,
    value_weight,
    pool_in_weight,
    log_gates,
    pool_weight,
    pool_scale,
    attention_out,
    pooling_out,
    final_gain,
):
    tok_rows = tokens.shape[0]
    width = query_weight.shape[0]
    groups = pool_weight.shape[0]
    head_size = pool_weight.shape[1]
    heads = log_gates.shape[0]
    attention_width = query_weight.shape[1]
    pool_width = pool_in_weight.shape[1]
    devices = lax.axis_size("sp")
    shards = lax.axis_size("tp")
    sequence_index = lax.axis_index("sp")
    first_row = sequence_index * tok_rows
    if shards == 2 and groups % 4 == 0 and heads % 2 == 0 and devices == 4 * heads and attention_width == pool_width:
        return layer(
            tokens, input_gain, query_weight, key_weight, value_weight, pool_in_weight, log_gates,
            pool_weight, pool_scale, attention_out, pooling_out, final_gain,
        )

    part = gathered(tokens, "tp")
    gain_part = gathered(input_gain.reshape(1, -1), "tp")
    widened = part.astype(jnp.float32)
    scaled = (widened * gain_part.astype(jnp.float32)).astype(jnp.bfloat16)

    def product(weight):
        return jnp.dot(scaled, weight, preferred_element_type=jnp.float32)

    inverse = lax.rsqrt(jnp.sum(widened * widened, axis=1) / width + epsilon)[:, None]
    keys = (product(key_weight) * inverse).astype(jnp.bfloat16)
    values = (product(value_weight) * inverse).astype(jnp.bfloat16)
    query = (product(query_weight) * (inverse * (LOG2E * head_size ** (-0.5)))).astype(jnp.bfloat16)
    pool_input = (product(pool_in_weight) * inverse).astype(jnp.bfloat16)
    rim = passed_along(pool_input[tok_rows - (WINDOW_MAX - 1) :], "sp", 1)

    attended = ring_attend(query, keys, values, log_gates)

    extended = jnp.concatenate([rim, pool_input], axis=0).astype(jnp.float32)
    column = jnp.arange(pool_width, dtype=jnp.int32)
    group_number = lax.axis_index("tp") * groups + column // head_size
    window = jnp.left_shift(jnp.full((pool_width,), 2, jnp.int32), group_number % 4)
    sums = extended
    span = 1
    chosen = jnp.zeros((tok_rows, pool_width), jnp.float32)
    for _ in range(4):
        sums = sums[span:] + sums[:-span]
        span = span * 2
        offset_rows = WINDOW_MAX - span
        chosen = jnp.where(window[None, :] == span, sums[offset_rows : offset_rows + tok_rows], chosen)
    element_locations = first_row + jnp.arange(tok_rows, dtype=jnp.int32)
    counts = jnp.minimum(window[None, :], element_locations[:, None] + 1).astype(jnp.float32)
    departure = (chosen / counts - pool_input.astype(jnp.float32)).astype(jnp.bfloat16)
    mapped = jnp.concatenate(
        [
            jnp.dot(
                departure[:, g * head_size : (g + 1) * head_size],
                pool_weight[g],
                preferred_element_type=jnp.float32,
            )
            for g in range(groups)
        ],
        axis=1,
    )
    pooled = (mapped * pool_scale).astype(jnp.bfloat16)
    pooled_part = jnp.dot(pooled, pooling_out, preferred_element_type=jnp.float32)
    whole = jnp.dot(attended, attention_out, preferred_element_type=jnp.float32) + pooled_part
    if shards == 2:
        half = width // 2
        lower = lax.axis_index("tp") == 0
        sent = jnp.where(lower, whole[:, half:], whole[:, :half]).astype(jnp.bfloat16)
        kept = jnp.where(lower, whole[:, :half], whole[:, half:])
        mixed = kept + swapped(sent, "tp", 1).astype(jnp.float32)
        squares = jnp.sum(mixed * mixed, axis=1)
        squares = squares + swapped(squares, "tp", 1)
    else:
        mixed = lax.psum_scatter(
            whole.astype(jnp.bfloat16), "tp", scatter_dimension=1, tiled=True
        ).astype(jnp.float32)
        squares = lax.psum(jnp.sum(mixed * mixed, axis=1), "tp")
    out_inverse = lax.rsqrt(squares / width + epsilon)
    return (mixed * out_inverse[:, None] * final_gain[None, :]).astype(jnp.bfloat16)


def solution(mesh):
    return jax.shard_map(
        body,
        mesh=mesh,
        in_specs=(
            P("sp", "tp"),
            P("tp"),
            P(None, "tp"),
            P(None, "tp"),
            P(None, "tp"),
            P(None, "tp"),
            P("tp", None),
            P("tp", None, None),
            P("tp"),
            P("tp", None),
            P("tp", None),
            P("tp"),
        ),
        out_specs=P("sp", "tp"),
        check_vma=False,
    )
```

```python
import functools

import jax
import jax.numpy as jnp
from jax import lax
from jax.experimental import pallas as pl
from jax.experimental.pallas import tpu as pltpu
from jax.sharding import PartitionSpec as P


WINDOW_MAX = 16
LANES = 128
LOG2E = 1.4426950408889634

very_low = -1e30
epsilon = 1e-06


def passed_along(block, axis, distance):
    devices = range(lax.axis_size(axis))
    route = [(i - distance, i) for i in devices if i - distance in devices]
    return lax.ppermute(block, axis, route)


def swapped(block, axis, offset):
    return lax.ppermute(block, axis, [(i, i ^ offset) for i in range(lax.axis_size(axis))])


def attend_kernel(first, last, heads, head_size, chunk, mode_ref, start_ref, *refs):
    if first:
        q_ref, kv_ref, gate_ref, acc_out, ml_out = refs
    else:
        q_ref, kv_ref, gate_ref, acc_in, ml_in, acc_out, ml_out = refs
    slot = pl.program_id(0)
    rows = q_ref.shape[1]
    keys = kv_ref.shape[0]
    width = heads * head_size
    lane = lax.broadcasted_iota(jnp.int32, (chunk, LANES), 1)

    def state_of(r, h):
        if first:
            return None
        ml = ml_in[0, r : r + chunk, :]
        columns = slice(h * head_size, (h + 1) * head_size)
        return (ml[:, h : h + 1], ml[:, heads + h : heads + h + 1], acc_in[0, r : r + chunk, columns])

    def store(r, h, ml, state):
        columns = slice(h * head_size, (h + 1) * head_size)
        high, total, summed = state
        if last:
            safe = jnp.where(total > 0.0, total, 1.0)
            acc_out[0, r : r + chunk, columns] = (summed / safe).astype(acc_out.dtype)
            level = jnp.where(total > 0.0, high + jnp.log2(safe), very_low)
            return jnp.where(lane == h, level, ml)
        acc_out[0, r : r + chunk, columns] = summed
        return jnp.where(lane == h, high, jnp.where(lane == heads + h, total, ml))

    def compute(diagonal):
        for r in range(0, rows, chunk):
            ml = jnp.zeros((chunk, LANES), jnp.float32)
            span = min(r + chunk, keys) if diagonal else keys
            for h in range(heads):
                columns = slice(h * head_size, (h + 1) * head_size)
                q = q_ref[0, r : r + chunk, columns]
                k = kv_ref[:span, columns]
                v = kv_ref[:span, width + h * head_size : width + (h + 1) * head_size]
                bias = (start_ref[slot * heads + h] - gate_ref[h : h + 1, :span]) * LOG2E
                s = lax.dot_general(q, k, (((1,), (1,)), ((), ())), preferred_element_type=jnp.float32)
                s = s + bias
                if diagonal:
                    row = r + lax.broadcasted_iota(jnp.int32, s.shape, 0)
                    s = jnp.where(row >= lax.broadcasted_iota(jnp.int32, s.shape, 1), s, very_low)
                old = state_of(r, h)
                high = jnp.max(s, axis=1, keepdims=True)
                if old is not None:
                    high = jnp.maximum(high, old[0])
                p = jnp.exp2(s - high)
                total = jnp.sum(p, axis=1, keepdims=True)
                summed = jnp.dot(p.astype(jnp.bfloat16), v, preferred_element_type=jnp.float32)
                if old is not None:
                    factor = jnp.exp2(old[0] - high)
                    total = total + factor * old[1]
                    summed = summed + factor * old[2]
                ml = store(r, h, ml, (high, total, summed))
            ml_out[0, r : r + chunk, :] = ml

    if first:
        pl.when(slot == 0)(lambda: compute(True))

        @pl.when((slot > 0) & (mode_ref[slot] > 0))
        def _():
            compute(False)

    else:

        @pl.when(mode_ref[slot] > 0)
        def _():
            compute(False)

    @pl.when((mode_ref[slot] == 0) & ((slot > 0) | (not first)))
    def _():
        for r in range(0, rows, chunk):
            ml = jnp.zeros((chunk, LANES), jnp.float32)
            for h in range(heads):
                old = state_of(r, h)
                if old is None:
                    old = (
                        jnp.full((chunk, 1), very_low, jnp.float32),
                        jnp.zeros((chunk, 1), jnp.float32),
                        jnp.zeros((chunk, head_size), jnp.float32),
                    )
                ml = store(r, h, ml, old)
            ml_out[0, r : r + chunk, :] = ml


def attend_step(mode, starts, queries, pair, gates, state, last, head_size):
    slots, rows, width = queries.shape
    heads = width // head_size
    first = state is None
    chunk = min(rows, 256)
    by_slot = lambda g, *_: (g, 0, 0)
    whole = lambda g, *_: (0, 0)
    in_specs = [
        pl.BlockSpec((1, rows, width), by_slot),
        pl.BlockSpec(pair.shape, whole),
        pl.BlockSpec(gates.shape, whole),
    ]
    state_specs = [pl.BlockSpec((1, rows, width), by_slot), pl.BlockSpec((1, rows, LANES), by_slot)]
    if not first:
        in_specs = in_specs + state_specs
    keys = pair.shape[0]
    return pl.pallas_call(
        functools.partial(attend_kernel, first, last, heads, head_size, chunk),
        out_shape=(
            jax.ShapeDtypeStruct((slots, rows, width), jnp.bfloat16 if last else jnp.float32),
            jax.ShapeDtypeStruct((slots, rows, LANES), jnp.float32),
        ),
        grid_spec=pltpu.PrefetchScalarGridSpec(
            num_scalar_prefetch=2, grid=(slots,), in_specs=in_specs, out_specs=state_specs
        ),
        compiler_params=pltpu.CompilerParams(dimension_semantics=("arbitrary",)),
        cost_estimate=pl.CostEstimate(
            flops=8 * slots * rows * keys * width,
            bytes_accessed=12 * slots * rows * width,
            transcendentals=slots * rows * keys * heads,
        ),
    )(mode, starts, queries, pair, gates, *(() if first else state))


MESH = pl.DeviceIdType.MESH
SUB_ROWS = 128
PIECES = 2


def layer_kernel(
    tokens_ref, gain_ref, query_weight, key_weight, value_weight, pool_in_weight, gate_ref,
    pool_weight_ref, pool_scale_ref, attention_out, pooling_out, final_gain_ref, out_ref,
    held_tokens, weights, outs, halves, norms, inverse, made, parts, rim, pool_input, extended, pooled, whole, foreign, row_sums,
    pairs, other_gates, gate_row, queries, results, attended, acc, high,
    w_sem, c_send, c_recv, e_send, e_recv, p_send, p_recv, rim_send, rim_recv,
    q_send, q_recv, t_send, t_recv, y_send, y_recv, s_send, s_recv, f_send, f_recv, o_send, o_recv,
):
    planes, rows, head_size = queries.shape
    width = 2 * halves.shape[2]
    half = width // 2
    inner = made.shape[2]
    groups = pool_weight_ref.shape[0]
    me, core = lax.axis_index("sp"), lax.axis_index("tp")
    devices = lax.axis_size("sp")
    seats = devices // planes
    plane, seat = me // seats, me % seats
    line, side = seat // 2, seat % 2
    maker = plane % 2
    reach = planes - 1
    span = seats * rows

    tokens_load = pltpu.make_async_copy(tokens_ref, held_tokens, w_sem.at[6])
    tokens_load.start()
    loads = [
        pltpu.make_async_copy(source, target, w_sem.at[n])
        for n, (source, target) in enumerate(
            [
                (key_weight, weights.at[0]), (value_weight, weights.at[1]), (query_weight, weights.at[2]),
                (pool_in_weight, weights.at[3]), (pooling_out, outs.at[0]), (attention_out, outs.at[1]),
            ]
        )
    ]
    for load in loads:
        load.start()

    def device(p, y, x, c):
        return {"sp": p * seats + 2 * y + x, "tp": c}

    sibling = {"tp": 1 - core}

    def columns(l):
        return pl.ds(pl.multiple_of(l * head_size, head_size), head_size)

    def kept(p, x):
        return 2 * (p // 2) + x

    own = kept(plane, side)

    def away(p, x, c):
        return (p != plane) | (x != side) | (c != core)

    def block_rows(p, y, x):
        return pl.ds(pl.multiple_of((p * seats + 2 * y + x) * rows, rows), rows)

    piece = rows // PIECES

    def block(t, p, y, x, h):
        at = pl.multiple_of((p * seats + 2 * y + x) * rows + h * piece, piece)
        return pairs.at[t, pl.ds(at, piece), pl.ds(0, head_size)]

    def copy(source, target, send, recv, to):
        return pltpu.make_async_remote_copy(
            src_ref=source, dst_ref=target, send_sem=send, recv_sem=recv, device_id=to, device_id_type=MESH
        )

    def arrival(target, recv):
        copy(target, target, q_send.at[0], recv, sibling).wait_recv()

    barrier = pltpu.get_barrier_semaphore()

    def greet(to):
        pl.semaphore_signal(barrier, inc=1, device_id=to, device_id_type=MESH)

    for p in range(planes):
        for x in range(2):
            for c in range(2):
                pl.when(away(p, x, c))(functools.partial(greet, device(p, line, x, c)))
    greet(device(plane, 1 - line, side, core))
    greet({"sp": (me + 1) % devices})
    greet({"sp": (me + devices - 1) % devices})

    def scale_rows(n, carry):
        at = pl.ds(pl.multiple_of(n * SUB_ROWS, SUB_ROWS), SUB_ROWS)
        widened = held_tokens[at, :].astype(jnp.float32)
        halves[core, at, :] = (widened * gain_ref[...].astype(jnp.float32).reshape(1, half)).astype(jnp.bfloat16)
        square = widened * widened
        norms[core, at, :] = functools.reduce(
            jnp.add, [square[:, c : c + LANES] for c in range(0, half, LANES)]
        )
        return carry

    tokens_load.wait()
    lax.fori_loop(0, rows // SUB_ROWS, scale_rows, 0)
    pl.semaphore_wait(barrier, 4 * planes + 2)

    swaps = (
        copy(halves.at[core], halves.at[core], c_send.at[0], c_recv.at[0], sibling),
        copy(norms.at[core], norms.at[core], c_send.at[1], c_recv.at[1], sibling),
        copy(gate_ref, other_gates, c_send.at[2], c_recv.at[2], sibling),
    )
    for c in swaps:
        c.start()

    def project(use):
        def one(c, carry):
            use(pl.ds(pl.multiple_of(c * 2 * LANES, 2 * LANES), 2 * LANES))
            return carry

        lax.fori_loop(0, inner // (2 * LANES), one, 0)

    def product(h, n, at):
        here = pl.ds(pl.multiple_of(h * half, half), half)
        return jnp.dot(halves[h], weights[n, here, at], preferred_element_type=jnp.float32)

    for n in range(3):
        loads[n].wait()

        def begin(at):
            parts[n, :, at] = product(core, n, at)

        project(begin)
    pairs[1, :, head_size:] = jnp.ones((pairs.shape[1], head_size), pairs.dtype)
    arrival(norms.at[1 - core], c_recv.at[1])
    total = jnp.sum(norms[0] + norms[1], axis=1, keepdims=True)
    inverse[...] = jnp.broadcast_to(lax.rsqrt(total / width + epsilon), inverse.shape)
    arrival(halves.at[1 - core], c_recv.at[0])

    def scaled_by(factor, r):
        f = inverse[...] * factor
        return (r * jnp.concatenate([f, f], axis=1)).astype(jnp.bfloat16)

    def complete(n, factor):
        def use(at):
            made[n, :, at] = scaled_by(factor, parts[n, :, at] + product(1 - core, n, at))

        project(use)

    def start_all(copies):
        for c in copies:
            c.start()

    def query_copy(p, x):
        l = kept(p, x)
        return copy(
            made.at[2, :, columns(l)], queries.at[plane], q_send.at[l], q_recv.at[plane], device(p, line, x, side)
        )

    def tensor_copies(t, p, x):
        l = kept(p, x)
        return [
            copy(
                made.at[t, pl.ds(h * piece, piece), columns(l)], block(t, plane, line, side, h),
                t_send.at[t, l, h], t_recv.at[2 * plane + side, h], device(p, line, x, t),
            )
            for h in range(PIECES)
        ]

    served = [2 * n + core for n in range(planes // 2)]
    middle = planes // 2
    upper = plane >= middle

    def crossing(p):
        return (p >= middle) != upper

    def wait_all(copies):
        for c in copies:
            c.wait_send()

    def send_tensor(t, p, wanted):
        for x in (side, 1 - side):
            pl.when(wanted & away(p, x, t))(lambda: start_all(tensor_copies(t, p, x)))

    def send_query(p, wanted):
        for x in (side, 1 - side):
            pl.when(wanted & away(p, x, side))(lambda: query_copy(p, x).start())

    def onward(p, x, h, source=None):
        n = 2 * p + x
        target = block(core, p, line, x, h)
        source = target if source is None else source
        return (
            copy(source, target, y_send.at[n, h], y_recv.at[n, h], device(plane, 1 - line, side, core)),
            copy(source, target, s_send.at[n, h], s_recv.at[n, h], sibling),
        )

    def onward_own():
        for h in range(PIECES):
            start_all(onward(plane, side, h, made.at[core, pl.ds(h * piece, piece), columns(own)]))

    mine = maker == core
    complete(0, 1.0)
    for p in served:
        send_tensor(0, p, p == plane)
    send_tensor(0, served[0], served[0] > plane)
    complete(1, 1.0)
    for p in served:
        send_tensor(1, p, p == plane)
    pl.when(mine)(onward_own)
    send_tensor(1, served[0], served[0] > plane)
    for p in served[1:]:
        send_tensor(0, p, p > plane)
        send_tensor(1, p, p > plane)
    complete(2, LOG2E * head_size ** (-0.5))
    for p in served:
        send_query(p, jnp.logical_not(crossing(p)) | upper)
    for p in served:
        for t in range(2):
            send_tensor(t, p, (p < plane) & jnp.logical_not(crossing(p)))

    for p in served:
        send_query(p, crossing(p) & jnp.logical_not(upper))

    def over_crossing(action):
        for p in served:
            for x in (side, 1 - side):
                pl.when(crossing(p))(functools.partial(action, p, x))

    def release_keys():
        def action(p, x):
            query_copy(p, x).wait_send()
            start_all(tensor_copies(0, p, x))

        over_crossing(action)

    def release_values():
        def action(p, x):
            wait_all(tensor_copies(0, p, x))
            start_all(tensor_copies(1, p, x))

        over_crossing(action)

    @pl.when(mine)
    def _():
        pairs[core, block_rows(plane, line, side), :head_size] = made[core, :, columns(own)]

    @pl.when(mine & (side == core))
    def _():
        queries[plane] = made[2, :, columns(own)]

    arrival(other_gates, c_recv.at[2])
    gates = jnp.where(mine, gate_ref[...], other_gates[...])
    chosen = lax.broadcasted_iota(jnp.int32, gates.shape, 0) == own
    gate_row[...] = jnp.sum(jnp.where(chosen, gates, 0.0), axis=0, keepdims=True)
    acc[...] = jnp.zeros_like(acc)
    high[...] = jnp.full_like(high, very_low)

    loads[3].wait()

    def pool_product(at):
        pool_input[:, at] = scaled_by(1.0, product(0, 3, at) + product(1, 3, at))

    project(pool_product)
    rim_copy = copy(
        pool_input.at[pl.ds(rows - WINDOW_MAX, WINDOW_MAX), :], rim, rim_send, rim_recv, {"sp": (me + 1) % devices}
    )
    rim_copy.start()

    def forward(p):
        for x in (side, 1 - side):

            @pl.when(jnp.logical_not(mine & (p == plane) & (x == side)))
            def _():
                for h in range(PIECES):
                    arrival(block(core, p, line, x, h), t_recv.at[2 * p + x, h])
                    start_all(onward(p, x, h))

    def beside(p, x, h):
        n = 2 * p + x
        held = block(core, p, 1 - line, x, h)
        return copy(held, held, f_send.at[n, h], f_recv.at[n, h], sibling)

    def relay(p):
        for x in (side, 1 - side):
            for h in range(PIECES):
                arrival(block(core, p, 1 - line, x, h), y_recv.at[2 * p + x, h])
                beside(p, x, h).start()

    def settle(p):
        for x in range(2):
            for h in range(PIECES):
                arrival(block(1 - core, p, line, x, h), s_recv.at[2 * p + x, h])
                arrival(block(1 - core, p, 1 - line, x, h), f_recv.at[2 * p + x, h])

    place = 2 * line + core

    def update(i, p, masked):
        here = pl.ds(pl.multiple_of(p * span, span), span)
        k = pairs[0, here, :head_size]
        v = pairs[1, here, :]
        gates = gate_row[:, here]
        start = gate_row[:, pl.ds(pl.multiple_of((i * seats + place) * rows, rows), LANES)][:, :1]
        bias = (start - gates) * LOG2E
        scores = []
        for r in range(0, rows, SUB_ROWS):
            q = queries[i, r : r + SUB_ROWS, :]
            s = lax.dot_general(q, k, (((1,), (1,)), ((), ())), preferred_element_type=jnp.float32) + bias
            if masked:
                row = place * rows + r + lax.broadcasted_iota(jnp.int32, s.shape, 0)
                s = jnp.where(row >= lax.broadcasted_iota(jnp.int32, s.shape, 1), s, very_low)
            scores.append(s)
        for n, r in enumerate(range(0, rows, SUB_ROWS)):
            s = scores[n]
            at = pl.ds(r, SUB_ROWS)
            old = high[i, at, :]
            new = jnp.maximum(old, jnp.max(s, axis=1, keepdims=True))
            p_ = jnp.exp2(s - new[:, :1]).astype(jnp.bfloat16)
            factor = jnp.exp2(old - new)
            summed = jnp.dot(p_, v, preferred_element_type=jnp.float32)
            acc[i, at, :] = acc[i, at, :] * jnp.concatenate([factor, factor], axis=1) + summed
            high[i, at, :] = new

    def finished(i):
        return copy(
            results.at[i], attended.at[maker, :, columns(own)], o_send.at[i], o_recv.at[own], device(i, line, core, maker)
        )

    def query_arrival(i):
        pl.when(away(i, core, maker))(lambda: arrival(queries.at[i], q_recv.at[i]))

    def result_of(i):
        return (acc[i, :, :head_size] / acc[i, :, head_size:]).astype(jnp.bfloat16)

    def give_back(i):
        @pl.when(away(i, core, maker))
        def _():
            results[i] = result_of(i)
            finished(i).start()

        @pl.when(jnp.logical_not(away(i, core, maker)))
        def _():
            attended[core, :, columns(own)] = result_of(i)

    def source(n):
        base = plane // middle * middle
        near = base + (plane - base + n) % middle
        return jnp.where(n < middle, near, jnp.where(upper, reach - n, n))

    pooled_copy = copy(pooled.at[core], pooled.at[core], e_send.at[0], e_recv.at[0], sibling)

    def pool():
        arrival(rim, rim_recv)

        for g in range(groups):
            at = slice(g * head_size, (g + 1) * head_size)
            window = 2 << (g % 4)
            before = jnp.where(me > 0, rim[:, at].astype(jnp.float32), 0.0)
            current = pool_input[:, at].astype(jnp.float32)
            extended[:WINDOW_MAX, :] = before
            extended[WINDOW_MAX:, :] = current
            depth = 1
            while depth < window:
                total = extended[depth:, :] + extended[: WINDOW_MAX + rows - depth, :]
                extended[depth:, :] = total
                depth = 2 * depth
            location = me * rows + lax.broadcasted_iota(jnp.int32, (rows, head_size), 0)
            count = jnp.minimum(window, location + 1).astype(jnp.float32)
            departure = (extended[WINDOW_MAX:, :] / count - current).astype(jnp.bfloat16)
            mapped = jnp.dot(departure, pool_weight_ref[g], preferred_element_type=jnp.float32)
            pooled[core, :, at] = (mapped * pool_scale_ref[:, at]).astype(jnp.bfloat16)

        pooled_copy.start()

    def step(n, carry):
        p = source(n)
        late = n == middle - 1
        more = n < reach
        relay(p)
        pl.when(upper & (n == 0))(release_keys)
        pl.when(more & jnp.logical_not(late))(lambda: forward(source(n + 1)))
        settle(p)

        def one(i, carry):
            pl.when(n == 0)(lambda: query_arrival(i))
            pl.when(i > p)(lambda: update(i, p, False))
            pl.when(i == p)(lambda: update(i, p, True))
            pl.when((i > plane) & jnp.where(upper, n == reach, i == p))(lambda: give_back(i))
            return carry

        lax.fori_loop(jnp.where(p > plane, p, plane), planes, one, 0)
        pl.when(upper & (n == middle - 1))(release_values)
        pl.when(more & late)(lambda: forward(source(n + 1)))
        return carry

    forward(plane)
    loads[4].wait()
    loads[5].wait()
    theirs = pl.ds(pl.multiple_of((1 - core) * half, half), half)
    shared = [copy(outs.at[n, :, theirs], foreign.at[n], e_send.at[2 + n], e_recv.at[2 + n], sibling) for n in range(2)]
    start_all(shared)
    lax.fori_loop(0, planes, step, 0)

    def serve(i, carry):
        query_arrival(i)

        def earlier(p, carry):
            update(i, p, False)
            return carry

        lax.fori_loop(0, i, earlier, 0)
        update(i, i, True)
        give_back(i)
        return carry

    lax.fori_loop(0, plane, serve, 0)
    give_back(plane)
    pool()

    chunks = half // (2 * LANES)

    def chunk_columns(c):
        return pl.ds(pl.multiple_of(c * 2 * LANES, 2 * LANES), 2 * LANES)

    def home_columns(c):
        return pl.ds(pl.multiple_of(core * half + c * 2 * LANES, 2 * LANES), 2 * LANES)

    for n in range(2):
        arrival(foreign.at[n], e_recv.at[2 + n])

    def pool_part(c, carry):
        at = chunk_columns(c)
        whole[:, at] = jnp.dot(pooled[core], outs[0, :, home_columns(c)], preferred_element_type=jnp.float32)
        return carry

    def pool_rest(c, carry):
        at = chunk_columns(c)
        r = jnp.dot(pooled[1 - core], foreign[0, :, at], preferred_element_type=jnp.float32)
        whole[:, at] = whole[:, at] + r
        return carry

    lax.fori_loop(0, chunks, pool_part, 0)
    arrival(pooled.at[1 - core], e_recv.at[0])
    lax.fori_loop(0, chunks, pool_rest, 0)

    def pass_on(l):
        held = attended.at[core, :, columns(l)]
        return copy(held, held, p_send.at[l], p_recv.at[l], sibling)

    for p in served:
        for x in range(2):
            l = kept(p, x)
            pl.when(away(p, x, side))(lambda: arrival(attended.at[core, :, columns(l)], o_recv.at[l]))
            pass_on(l).start()

    def retain(c, carry):
        at = chunk_columns(c)
        r = jnp.dot(attended[core], outs[1, :, home_columns(c)], preferred_element_type=jnp.float32)
        whole[:, at] = whole[:, at] + r
        return carry

    lax.fori_loop(0, chunks, retain, 0)
    for l in range(planes):
        arrival(attended.at[1 - core, :, columns(l)], p_recv.at[l])

    def add(c, carry):
        at = chunk_columns(c)
        r = jnp.dot(attended[1 - core], foreign[1, :, at], preferred_element_type=jnp.float32)
        whole[:, at] = whole[:, at] + r
        return carry

    lax.fori_loop(0, chunks, add, 0)

    def square_rows(n, carry):
        at = pl.ds(pl.multiple_of(n * SUB_ROWS, SUB_ROWS), SUB_ROWS)
        mixed = whole[at, :]
        square = mixed * mixed
        row_sums[core, at, :] = functools.reduce(
            jnp.add, [square[:, c : c + LANES] for c in range(0, half, LANES)]
        )
        return carry

    lax.fori_loop(0, rows // SUB_ROWS, square_rows, 0)
    sums = copy(row_sums.at[core], row_sums.at[core], e_send.at[1], e_recv.at[1], sibling)
    sums.start()
    arrival(row_sums.at[1 - core], e_recv.at[1])

    def finish_rows(n, carry):
        at = pl.ds(pl.multiple_of(n * SUB_ROWS, SUB_ROWS), SUB_ROWS)
        total = jnp.sum(row_sums[0, at, :] + row_sums[1, at, :], axis=1, keepdims=True)
        out_inverse = lax.rsqrt(total / width + epsilon)
        out_ref[at, :] = (whole[at, :] * out_inverse * final_gain_ref[...]).astype(jnp.bfloat16)
        return carry

    lax.fori_loop(0, rows // SUB_ROWS, finish_rows, 0)

    for p in served:
        for x in range(2):
            waited = crossing(p)
            left = (
                (lambda: query_copy(p, x).wait_send(), waited & upper, side),
                (lambda: wait_all(tensor_copies(0, p, x)), waited & upper, 0),
                (lambda: wait_all(tensor_copies(1, p, x)), False, 1),
            )
            for action, done, c in left:
                pl.when(away(p, x, c) & jnp.logical_not(done))(action)
    for p in range(planes):
        for x in range(2):
            for h in range(PIECES):
                for c in onward(p, x, h):
                    c.wait_send()
                beside(p, x, h).wait_send()
        pl.when(away(p, core, maker))(lambda: finished(p).wait_send())
    for c in [*swaps, *shared, rim_copy, pooled_copy, sums] + [pass_on(l) for l in range(planes)]:
        c.wait_send()


def layer(
    tokens, input_gain, query_weight, key_weight, value_weight, pool_in_weight, log_gates,
    pool_weight, pool_scale, attention_out, pooling_out, final_gain,
):
    rows, half = tokens.shape
    width, inner = query_weight.shape
    planes = log_gates.shape[0]
    head_size = pool_weight.shape[1]
    blocks = lax.axis_size("sp")
    dma = pltpu.SemaphoreType.DMA
    tile = lambda *shape: pltpu.VMEM(shape, jnp.bfloat16)
    wide = lambda *shape: pltpu.VMEM(shape, jnp.float32)
    near = pl.BlockSpec(memory_space=pltpu.VMEM)
    away = pl.BlockSpec(memory_space=pl.ANY)
    pairs = blocks * (blocks + 1) // 2
    return pl.pallas_call(
        layer_kernel,
        out_shape=jax.ShapeDtypeStruct((rows, half), jnp.bfloat16),
        in_specs=[away, near, away, away, away, away, near, near, near, away, away, near],
        out_specs=near,
        scratch_shapes=[
            tile(rows, half), tile(4, width, inner), tile(2, inner, width), tile(2, rows, half), wide(2, rows, LANES),
            wide(rows, LANES), tile(3, rows, inner), wide(3, rows, inner), tile(WINDOW_MAX, inner), tile(rows, inner),
            wide(WINDOW_MAX + rows, head_size), tile(2, rows, inner), wide(rows, half),
            tile(2, inner, half), wide(2, rows, LANES),
            tile(2, blocks * rows, 2 * head_size), wide(*log_gates.shape), wide(1, blocks * rows),
            tile(planes, rows, head_size), tile(planes, rows, head_size), tile(2, rows, inner),
            wide(planes, rows, 2 * head_size), wide(planes, rows, LANES),
            dma((7,)), dma((3,)), dma((3,)), dma((4,)), dma((4,)), dma((planes,)), dma((planes,)), dma, dma,
            dma((planes,)), dma((planes,)),
            dma((2, planes, PIECES)), dma((2 * planes, PIECES)),
            dma((2 * planes, PIECES)), dma((2 * planes, PIECES)),
            dma((2 * planes, PIECES)), dma((2 * planes, PIECES)),
            dma((2 * planes, PIECES)), dma((2 * planes, PIECES)),
            dma((planes,)), dma((planes,)),
        ],
        compiler_params=pltpu.CompilerParams(
            collective_id=0, has_side_effects=True, vmem_limit_bytes=56 * 2**20
        ),
        cost_estimate=pl.CostEstimate(
            flops=4 * pairs * rows * rows * head_size + 12 * rows * width * inner,
            bytes_accessed=12 * width * inner,
            transcendentals=pairs * rows * rows,
        ),
    )(
        tokens, input_gain, query_weight, key_weight, value_weight, pool_in_weight, log_gates,
        pool_weight, pool_scale.reshape(1, -1), attention_out, pooling_out, final_gain.reshape(1, -1),
    )


def ring_attend(query, keys, values, log_gates):
    tok_rows = query.shape[0]
    heads = log_gates.shape[0]
    head_size = query.shape[1] // heads
    devices = lax.axis_size("sp")
    side = 1
    while (2 * side) ** 2 <= devices and devices % (2 * side) == 0:
        side = 2 * side
    planes = devices // side
    sequence_index = lax.axis_index("sp")
    plane = sequence_index // side
    seat = sequence_index % side
    pair = jnp.concatenate([keys, values], axis=1)
    pairs = [pair]
    for _ in range(1, planes):
        pairs.append(passed_along(pairs[-1], "sp", side))
    queries = jnp.stack([query] + [swapped(query, "sp", g) for g in range(1, side)])
    seats = seat ^ jnp.arange(side, dtype=jnp.int32)
    starts = jnp.stack(
        [
            lax.dynamic_slice_in_dim(log_gates, (plane * side + (seat ^ g)) * tok_rows, 1, 1)[:, 0]
            for g in range(side)
        ]
    ).reshape(-1)
    state = None
    for k in range(planes):
        source = jnp.maximum(sequence_index - k * side, seat)
        gates = lax.dynamic_slice_in_dim(log_gates, source * tok_rows, tok_rows, 1)
        if k == 0:
            mode = (seats > seat).astype(jnp.int32)
        else:
            mode = jnp.full((side,), plane >= k, jnp.int32)
        state = attend_step(
            mode, starts, queries, pairs[k], gates, state, k == planes - 1, head_size
        )
    partial, level = state
    level = level[:, :, :heads]
    shares = [partial[0]] + [swapped(partial[g], "sp", g) for g in range(1, side)]
    tall = jnp.transpose(level, (0, 2, 1))
    levels = jnp.stack([tall[0]] + [swapped(tall[g], "sp", g) for g in range(1, side)])
    portion = jnp.exp2(levels - jnp.max(levels, axis=0, keepdims=True))
    portion = portion / jnp.sum(portion, axis=0, keepdims=True)
    portion = jnp.transpose(portion, (0, 2, 1))
    attended = 0.0
    for g in range(side):
        attended = attended + shares[g].astype(jnp.float32) * jnp.repeat(portion[g], head_size, axis=1)
    return attended.astype(jnp.bfloat16)


def gathered(block, axis):
    if lax.axis_size(axis) != 2:
        return lax.all_gather(block, axis, axis=1, tiled=True)
    other = swapped(block, axis, 1)
    lower = lax.axis_index(axis) == 0
    return jnp.concatenate([jnp.where(lower, block, other), jnp.where(lower, other, block)], axis=1)


def body(
    tokens,
    input_gain,
    query_weight,
    key_weight,
    value_weight,
    pool_in_weight,
    log_gates,
    pool_weight,
    pool_scale,
    attention_out,
    pooling_out,
    final_gain,
):
    tok_rows = tokens.shape[0]
    width = query_weight.shape[0]
    groups = pool_weight.shape[0]
    head_size = pool_weight.shape[1]
    heads = log_gates.shape[0]
    attention_width = query_weight.shape[1]
    pool_width = pool_in_weight.shape[1]
    devices = lax.axis_size("sp")
    shards = lax.axis_size("tp")
    sequence_index = lax.axis_index("sp")
    first_row = sequence_index * tok_rows
    if shards == 2 and groups % 4 == 0 and heads % 2 == 0 and devices == 4 * heads and attention_width == pool_width:
        return layer(
            tokens, input_gain, query_weight, key_weight, value_weight, pool_in_weight, log_gates,
            pool_weight, pool_scale, attention_out, pooling_out, final_gain,
        )

    part = gathered(tokens, "tp")
    gain_part = gathered(input_gain.reshape(1, -1), "tp")
    widened = part.astype(jnp.float32)
    scaled = (widened * gain_part.astype(jnp.float32)).astype(jnp.bfloat16)

    def product(weight):
        return jnp.dot(scaled, weight, preferred_element_type=jnp.float32)

    inverse = lax.rsqrt(jnp.sum(widened * widened, axis=1) / width + epsilon)[:, None]
    keys = (product(key_weight) * inverse).astype(jnp.bfloat16)
    values = (product(value_weight) * inverse).astype(jnp.bfloat16)
    query = (product(query_weight) * (inverse * (LOG2E * head_size ** (-0.5)))).astype(jnp.bfloat16)
    pool_input = (product(pool_in_weight) * inverse).astype(jnp.bfloat16)
    rim = passed_along(pool_input[tok_rows - (WINDOW_MAX - 1) :], "sp", 1)

    attended = ring_attend(query, keys, values, log_gates)

    extended = jnp.concatenate([rim, pool_input], axis=0).astype(jnp.float32)
    column = jnp.arange(pool_width, dtype=jnp.int32)
    group_number = lax.axis_index("tp") * groups + column // head_size
    window = jnp.left_shift(jnp.full((pool_width,), 2, jnp.int32), group_number % 4)
    sums = extended
    span = 1
    chosen = jnp.zeros((tok_rows, pool_width), jnp.float32)
    for _ in range(4):
        sums = sums[span:] + sums[:-span]
        span = span * 2
        offset_rows = WINDOW_MAX - span
        chosen = jnp.where(window[None, :] == span, sums[offset_rows : offset_rows + tok_rows], chosen)
    element_locations = first_row + jnp.arange(tok_rows, dtype=jnp.int32)
    counts = jnp.minimum(window[None, :], element_locations[:, None] + 1).astype(jnp.float32)
    departure = (chosen / counts - pool_input.astype(jnp.float32)).astype(jnp.bfloat16)
    mapped = jnp.concatenate(
        [
            jnp.dot(
                departure[:, g * head_size : (g + 1) * head_size],
                pool_weight[g],
                preferred_element_type=jnp.float32,
            )
            for g in range(groups)
        ],
        axis=1,
    )
    pooled = (mapped * pool_scale).astype(jnp.bfloat16)
    pooled_part = jnp.dot(pooled, pooling_out, preferred_element_type=jnp.float32)
    whole = jnp.dot(attended, attention_out, preferred_element_type=jnp.float32) + pooled_part
    if shards == 2:
        half = width // 2
        lower = lax.axis_index("tp") == 0
        sent = jnp.where(lower, whole[:, half:], whole[:, :half]).astype(jnp.bfloat16)
        kept = jnp.where(lower, whole[:, :half], whole[:, half:])
        mixed = kept + swapped(sent, "tp", 1).astype(jnp.float32)
        squares = jnp.sum(mixed * mixed, axis=1)
        squares = squares + swapped(squares, "tp", 1)
    else:
        mixed = lax.psum_scatter(
            whole.astype(jnp.bfloat16), "tp", scatter_dimension=1, tiled=True
        ).astype(jnp.float32)
        squares = lax.psum(jnp.sum(mixed * mixed, axis=1), "tp")
    out_inverse = lax.rsqrt(squares / width + epsilon)
    return (mixed * out_inverse[:, None] * final_gain[None, :]).astype(jnp.bfloat16)


def solution(mesh):
    return jax.shard_map(
        body,
        mesh=mesh,
        in_specs=(
            P("sp", "tp"),
            P("tp"),
            P(None, "tp"),
            P(None, "tp"),
            P(None, "tp"),
            P(None, "tp"),
            P("tp", None),
            P("tp", None, None),
            P("tp"),
            P("tp", None),
            P("tp", None),
            P("tp"),
        ),
        out_specs=P("sp", "tp"),
        check_vma=False,
    )
```

```python
import functools

import jax
import jax.numpy as jnp
from jax import lax
from jax.experimental import pallas as pl
from jax.experimental.pallas import tpu as pltpu
from jax.sharding import PartitionSpec as P


WINDOW_MAX = 16
LANES = 128
LOG2E = 1.4426950408889634

very_low = -1e30
epsilon = 1e-06


def passed_along(block, axis, distance):
    devices = range(lax.axis_size(axis))
    route = [(i - distance, i) for i in devices if i - distance in devices]
    return lax.ppermute(block, axis, route)


def swapped(block, axis, offset):
    return lax.ppermute(block, axis, [(i, i ^ offset) for i in range(lax.axis_size(axis))])


def attend_kernel(first, last, heads, head_size, chunk, mode_ref, start_ref, *refs):
    if first:
        q_ref, kv_ref, gate_ref, acc_out, ml_out = refs
    else:
        q_ref, kv_ref, gate_ref, acc_in, ml_in, acc_out, ml_out = refs
    slot = pl.program_id(0)
    rows = q_ref.shape[1]
    keys = kv_ref.shape[0]
    width = heads * head_size
    lane = lax.broadcasted_iota(jnp.int32, (chunk, LANES), 1)

    def state_of(r, h):
        if first:
            return None
        ml = ml_in[0, r : r + chunk, :]
        columns = slice(h * head_size, (h + 1) * head_size)
        return (ml[:, h : h + 1], ml[:, heads + h : heads + h + 1], acc_in[0, r : r + chunk, columns])

    def store(r, h, ml, state):
        columns = slice(h * head_size, (h + 1) * head_size)
        high, total, summed = state
        if last:
            safe = jnp.where(total > 0.0, total, 1.0)
            acc_out[0, r : r + chunk, columns] = (summed / safe).astype(acc_out.dtype)
            level = jnp.where(total > 0.0, high + jnp.log2(safe), very_low)
            return jnp.where(lane == h, level, ml)
        acc_out[0, r : r + chunk, columns] = summed
        return jnp.where(lane == h, high, jnp.where(lane == heads + h, total, ml))

    def compute(diagonal):
        for r in range(0, rows, chunk):
            ml = jnp.zeros((chunk, LANES), jnp.float32)
            span = min(r + chunk, keys) if diagonal else keys
            for h in range(heads):
                columns = slice(h * head_size, (h + 1) * head_size)
                q = q_ref[0, r : r + chunk, columns]
                k = kv_ref[:span, columns]
                v = kv_ref[:span, width + h * head_size : width + (h + 1) * head_size]
                bias = (start_ref[slot * heads + h] - gate_ref[h : h + 1, :span]) * LOG2E
                s = lax.dot_general(q, k, (((1,), (1,)), ((), ())), preferred_element_type=jnp.float32)
                s = s + bias
                if diagonal:
                    row = r + lax.broadcasted_iota(jnp.int32, s.shape, 0)
                    s = jnp.where(row >= lax.broadcasted_iota(jnp.int32, s.shape, 1), s, very_low)
                old = state_of(r, h)
                high = jnp.max(s, axis=1, keepdims=True)
                if old is not None:
                    high = jnp.maximum(high, old[0])
                p = jnp.exp2(s - high)
                total = jnp.sum(p, axis=1, keepdims=True)
                summed = jnp.dot(p.astype(jnp.bfloat16), v, preferred_element_type=jnp.float32)
                if old is not None:
                    factor = jnp.exp2(old[0] - high)
                    total = total + factor * old[1]
                    summed = summed + factor * old[2]
                ml = store(r, h, ml, (high, total, summed))
            ml_out[0, r : r + chunk, :] = ml

    if first:
        pl.when(slot == 0)(lambda: compute(True))

        @pl.when((slot > 0) & (mode_ref[slot] > 0))
        def _():
            compute(False)

    else:

        @pl.when(mode_ref[slot] > 0)
        def _():
            compute(False)

    @pl.when((mode_ref[slot] == 0) & ((slot > 0) | (not first)))
    def _():
        for r in range(0, rows, chunk):
            ml = jnp.zeros((chunk, LANES), jnp.float32)
            for h in range(heads):
                old = state_of(r, h)
                if old is None:
                    old = (
                        jnp.full((chunk, 1), very_low, jnp.float32),
                        jnp.zeros((chunk, 1), jnp.float32),
                        jnp.zeros((chunk, head_size), jnp.float32),
                    )
                ml = store(r, h, ml, old)
            ml_out[0, r : r + chunk, :] = ml


def attend_step(mode, starts, queries, pair, gates, state, last, head_size):
    slots, rows, width = queries.shape
    heads = width // head_size
    first = state is None
    chunk = min(rows, 256)
    by_slot = lambda g, *_: (g, 0, 0)
    whole = lambda g, *_: (0, 0)
    in_specs = [
        pl.BlockSpec((1, rows, width), by_slot),
        pl.BlockSpec(pair.shape, whole),
        pl.BlockSpec(gates.shape, whole),
    ]
    state_specs = [pl.BlockSpec((1, rows, width), by_slot), pl.BlockSpec((1, rows, LANES), by_slot)]
    if not first:
        in_specs = in_specs + state_specs
    keys = pair.shape[0]
    return pl.pallas_call(
        functools.partial(attend_kernel, first, last, heads, head_size, chunk),
        out_shape=(
            jax.ShapeDtypeStruct((slots, rows, width), jnp.bfloat16 if last else jnp.float32),
            jax.ShapeDtypeStruct((slots, rows, LANES), jnp.float32),
        ),
        grid_spec=pltpu.PrefetchScalarGridSpec(
            num_scalar_prefetch=2, grid=(slots,), in_specs=in_specs, out_specs=state_specs
        ),
        compiler_params=pltpu.CompilerParams(dimension_semantics=("arbitrary",)),
        cost_estimate=pl.CostEstimate(
            flops=8 * slots * rows * keys * width,
            bytes_accessed=12 * slots * rows * width,
            transcendentals=slots * rows * keys * heads,
        ),
    )(mode, starts, queries, pair, gates, *(() if first else state))


MESH = pl.DeviceIdType.MESH
SUB_ROWS = 128
PIECES = 2


def layer_kernel(
    tokens_ref, gain_ref, query_weight, key_weight, value_weight, pool_in_weight, gate_ref,
    pool_weight_ref, pool_scale_ref, attention_out, pooling_out, final_gain_ref, out_ref,
    held_tokens, finished_rows, weights, outs, halves, norms, inverse, made, parts, rim, pool_input, extended, pooled, whole, foreign, row_sums,
    pairs, other_gates, gate_row, queries, results, attended, acc, high,
    w_sem, f_sem, c_send, c_recv, e_send, e_recv, p_send, p_recv, rim_send, rim_recv,
    q_send, q_recv, t_send, t_recv, y_send, y_recv, s_send, s_recv, f_send, f_recv, o_send, o_recv,
):
    planes, rows, head_size = queries.shape
    width = 2 * halves.shape[2]
    half = width // 2
    inner = made.shape[2]
    groups = pool_weight_ref.shape[0]
    me, core = lax.axis_index("sp"), lax.axis_index("tp")
    devices = lax.axis_size("sp")
    seats = devices // planes
    plane, seat = me // seats, me % seats
    line, side = seat // 2, seat % 2
    maker = plane % 2
    reach = planes - 1
    span = seats * rows

    tokens_load = pltpu.make_async_copy(tokens_ref, held_tokens, w_sem.at[6])
    tokens_load.start()
    loads = [
        pltpu.make_async_copy(source, target, w_sem.at[n])
        for n, (source, target) in enumerate(
            [
                (key_weight, weights.at[0]), (value_weight, weights.at[1]), (query_weight, weights.at[2]),
                (pool_in_weight, weights.at[3]), (pooling_out, outs.at[0]), (attention_out, outs.at[1]),
            ]
        )
    ]
    for load in loads:
        load.start()

    def device(p, y, x, c):
        return {"sp": p * seats + 2 * y + x, "tp": c}

    sibling = {"tp": 1 - core}

    def columns(l):
        return pl.ds(pl.multiple_of(l * head_size, head_size), head_size)

    def kept(p, x):
        return 2 * (p // 2) + x

    own = kept(plane, side)

    def away(p, x, c):
        return (p != plane) | (x != side) | (c != core)

    def block_rows(p, y, x):
        return pl.ds(pl.multiple_of((p * seats + 2 * y + x) * rows, rows), rows)

    piece = rows // PIECES

    def block(t, p, y, x, h):
        at = pl.multiple_of((p * seats + 2 * y + x) * rows + h * piece, piece)
        return pairs.at[t, pl.ds(at, piece), pl.ds(0, head_size)]

    def copy(source, target, send, recv, to):
        return pltpu.make_async_remote_copy(
            src_ref=source, dst_ref=target, send_sem=send, recv_sem=recv, device_id=to, device_id_type=MESH
        )

    def arrival(target, recv):
        copy(target, target, q_send.at[0], recv, sibling).wait_recv()

    barrier = pltpu.get_barrier_semaphore()

    def greet(to):
        pl.semaphore_signal(barrier, inc=1, device_id=to, device_id_type=MESH)

    for p in range(planes):
        for x in range(2):
            for c in range(2):
                pl.when(away(p, x, c))(functools.partial(greet, device(p, line, x, c)))
    greet(device(plane, 1 - line, side, core))
    greet({"sp": (me + 1) % devices})
    greet({"sp": (me + devices - 1) % devices})

    def scale_rows(n, carry):
        at = pl.ds(pl.multiple_of(n * SUB_ROWS, SUB_ROWS), SUB_ROWS)
        widened = held_tokens[at, :].astype(jnp.float32)
        halves[core, at, :] = (widened * gain_ref[...].astype(jnp.float32).reshape(1, half)).astype(jnp.bfloat16)
        square = widened * widened
        norms[core, at, :] = functools.reduce(
            jnp.add, [square[:, c : c + LANES] for c in range(0, half, LANES)]
        )
        return carry

    tokens_load.wait()
    lax.fori_loop(0, rows // SUB_ROWS, scale_rows, 0)
    pl.semaphore_wait(barrier, 4 * planes + 2)

    swaps = (
        copy(halves.at[core], halves.at[core], c_send.at[0], c_recv.at[0], sibling),
        copy(norms.at[core], norms.at[core], c_send.at[1], c_recv.at[1], sibling),
        copy(gate_ref, other_gates, c_send.at[2], c_recv.at[2], sibling),
    )
    for c in swaps:
        c.start()

    def project(use):
        def one(c, carry):
            use(pl.ds(pl.multiple_of(c * 2 * LANES, 2 * LANES), 2 * LANES))
            return carry

        lax.fori_loop(0, inner // (2 * LANES), one, 0)

    def product(h, n, at):
        here = pl.ds(pl.multiple_of(h * half, half), half)
        return jnp.dot(halves[h], weights[n, here, at], preferred_element_type=jnp.float32)

    for n in range(3):
        loads[n].wait()

        def begin(at):
            parts[n, :, at] = product(core, n, at)

        project(begin)
    pairs[1, :, head_size:] = jnp.ones((pairs.shape[1], head_size), pairs.dtype)
    arrival(norms.at[1 - core], c_recv.at[1])
    total = jnp.sum(norms[0] + norms[1], axis=1, keepdims=True)
    inverse[...] = jnp.broadcast_to(lax.rsqrt(total / width + epsilon), inverse.shape)
    arrival(halves.at[1 - core], c_recv.at[0])

    def scaled_by(factor, r):
        f = inverse[...] * factor
        return (r * jnp.concatenate([f, f], axis=1)).astype(jnp.bfloat16)

    def complete(n, factor):
        def use(at):
            made[n, :, at] = scaled_by(factor, parts[n, :, at] + product(1 - core, n, at))

        project(use)

    def start_all(copies):
        for c in copies:
            c.start()

    def query_copy(p, x):
        l = kept(p, x)
        return copy(
            made.at[2, :, columns(l)], queries.at[plane], q_send.at[l], q_recv.at[plane], device(p, line, x, side)
        )

    def tensor_copies(t, p, x):
        l = kept(p, x)
        return [
            copy(
                made.at[t, pl.ds(h * piece, piece), columns(l)], block(t, plane, line, side, h),
                t_send.at[t, l, h], t_recv.at[2 * plane + side, h], device(p, line, x, t),
            )
            for h in range(PIECES)
        ]

    served = [2 * n + core for n in range(planes // 2)]
    middle = planes // 2
    upper = plane >= middle

    def crossing(p):
        return (p >= middle) != upper

    def wait_all(copies):
        for c in copies:
            c.wait_send()

    def send_tensor(t, p, wanted):
        for x in (side, 1 - side):
            pl.when(wanted & away(p, x, t))(lambda: start_all(tensor_copies(t, p, x)))

    def send_query(p, wanted):
        for x in (side, 1 - side):
            pl.when(wanted & away(p, x, side))(lambda: query_copy(p, x).start())

    def onward(p, x, h, source=None):
        n = 2 * p + x
        target = block(core, p, line, x, h)
        source = target if source is None else source
        return (
            copy(source, target, y_send.at[n, h], y_recv.at[n, h], device(plane, 1 - line, side, core)),
            copy(source, target, s_send.at[n, h], s_recv.at[n, h], sibling),
        )

    def onward_own():
        for h in range(PIECES):
            start_all(onward(plane, side, h, made.at[core, pl.ds(h * piece, piece), columns(own)]))

    mine = maker == core
    complete(0, 1.0)
    for p in served:
        send_tensor(0, p, p == plane)
    send_tensor(0, served[0], served[0] > plane)
    complete(1, 1.0)
    for p in served:
        send_tensor(1, p, p == plane)
    pl.when(mine)(onward_own)
    send_tensor(1, served[0], served[0] > plane)
    for p in served[1:]:
        send_tensor(0, p, p > plane)
        send_tensor(1, p, p > plane)
    complete(2, LOG2E * head_size ** (-0.5))
    for p in served:
        send_query(p, jnp.logical_not(crossing(p)) | upper)
    for p in served:
        for t in range(2):
            send_tensor(t, p, (p < plane) & jnp.logical_not(crossing(p)))

    for p in served:
        send_query(p, crossing(p) & jnp.logical_not(upper))

    def over_crossing(action):
        for p in served:
            for x in (side, 1 - side):
                pl.when(crossing(p))(functools.partial(action, p, x))

    def release_keys():
        def action(p, x):
            query_copy(p, x).wait_send()
            start_all(tensor_copies(0, p, x))

        over_crossing(action)

    def release_values():
        def action(p, x):
            wait_all(tensor_copies(0, p, x))
            start_all(tensor_copies(1, p, x))

        over_crossing(action)

    @pl.when(mine)
    def _():
        pairs[core, block_rows(plane, line, side), :head_size] = made[core, :, columns(own)]

    @pl.when(mine & (side == core))
    def _():
        queries[plane] = made[2, :, columns(own)]

    arrival(other_gates, c_recv.at[2])
    gates = jnp.where(mine, gate_ref[...], other_gates[...])
    chosen = lax.broadcasted_iota(jnp.int32, gates.shape, 0) == own
    gate_row[...] = jnp.sum(jnp.where(chosen, gates, 0.0), axis=0, keepdims=True)
    acc[...] = jnp.zeros_like(acc)
    high[...] = jnp.full_like(high, very_low)

    loads[3].wait()

    def pool_product(at):
        pool_input[:, at] = scaled_by(1.0, product(0, 3, at) + product(1, 3, at))

    project(pool_product)
    rim_copy = copy(
        pool_input.at[pl.ds(rows - WINDOW_MAX, WINDOW_MAX), :], rim, rim_send, rim_recv, {"sp": (me + 1) % devices}
    )
    rim_copy.start()

    def forward(p):
        for x in (side, 1 - side):

            @pl.when(jnp.logical_not(mine & (p == plane) & (x == side)))
            def _():
                for h in range(PIECES):
                    arrival(block(core, p, line, x, h), t_recv.at[2 * p + x, h])
                    start_all(onward(p, x, h))

    def beside(p, x, h):
        n = 2 * p + x
        held = block(core, p, 1 - line, x, h)
        return copy(held, held, f_send.at[n, h], f_recv.at[n, h], sibling)

    def relay(p):
        for x in (side, 1 - side):
            for h in range(PIECES):
                arrival(block(core, p, 1 - line, x, h), y_recv.at[2 * p + x, h])
                beside(p, x, h).start()

    def settle(p):
        for x in range(2):
            for h in range(PIECES):
                arrival(block(1 - core, p, line, x, h), s_recv.at[2 * p + x, h])
                arrival(block(1 - core, p, 1 - line, x, h), f_recv.at[2 * p + x, h])

    place = 2 * line + core

    def update(i, p, masked):
        here = pl.ds(pl.multiple_of(p * span, span), span)
        k = pairs[0, here, :head_size]
        v = pairs[1, here, :]
        gates = gate_row[:, here]
        start = gate_row[:, pl.ds(pl.multiple_of((i * seats + place) * rows, rows), LANES)][:, :1]
        bias = (start - gates) * LOG2E
        scores = []
        for r in range(0, rows, SUB_ROWS):
            q = queries[i, r : r + SUB_ROWS, :]
            s = lax.dot_general(q, k, (((1,), (1,)), ((), ())), preferred_element_type=jnp.float32) + bias
            if masked:
                row = place * rows + r + lax.broadcasted_iota(jnp.int32, s.shape, 0)
                s = jnp.where(row >= lax.broadcasted_iota(jnp.int32, s.shape, 1), s, very_low)
            scores.append(s)
        for n, r in enumerate(range(0, rows, SUB_ROWS)):
            s = scores[n]
            at = pl.ds(r, SUB_ROWS)
            old = high[i, at, :]
            new = jnp.maximum(old, jnp.max(s, axis=1, keepdims=True))
            p_ = jnp.exp2(s - new[:, :1]).astype(jnp.bfloat16)
            factor = jnp.exp2(old - new)
            summed = jnp.dot(p_, v, preferred_element_type=jnp.float32)
            acc[i, at, :] = acc[i, at, :] * jnp.concatenate([factor, factor], axis=1) + summed
            high[i, at, :] = new

    def finished(i):
        return copy(
            results.at[i], attended.at[maker, :, columns(own)], o_send.at[i], o_recv.at[own], device(i, line, core, maker)
        )

    def query_arrival(i):
        pl.when(away(i, core, maker))(lambda: arrival(queries.at[i], q_recv.at[i]))

    def result_of(i):
        return (acc[i, :, :head_size] / acc[i, :, head_size:]).astype(jnp.bfloat16)

    def give_back(i):
        @pl.when(away(i, core, maker))
        def _():
            results[i] = result_of(i)
            finished(i).start()

        @pl.when(jnp.logical_not(away(i, core, maker)))
        def _():
            attended[core, :, columns(own)] = result_of(i)

    def source(n):
        base = plane // middle * middle
        near = base + (plane - base + n) % middle
        return jnp.where(n < middle, near, jnp.where(upper, reach - n, n))

    pooled_copy = copy(pooled.at[core], pooled.at[core], e_send.at[0], e_recv.at[0], sibling)

    def pool():
        arrival(rim, rim_recv)

        for g in range(groups):
            at = slice(g * head_size, (g + 1) * head_size)
            window = 2 << (g % 4)
            before = jnp.where(me > 0, rim[:, at].astype(jnp.float32), 0.0)
            current = pool_input[:, at].astype(jnp.float32)
            extended[:WINDOW_MAX, :] = before
            extended[WINDOW_MAX:, :] = current
            depth = 1
            while depth < window:
                total = extended[depth:, :] + extended[: WINDOW_MAX + rows - depth, :]
                extended[depth:, :] = total
                depth = 2 * depth
            location = me * rows + lax.broadcasted_iota(jnp.int32, (rows, head_size), 0)
            count = jnp.minimum(window, location + 1).astype(jnp.float32)
            departure = (extended[WINDOW_MAX:, :] / count - current).astype(jnp.bfloat16)
            mapped = jnp.dot(departure, pool_weight_ref[g], preferred_element_type=jnp.float32)
            pooled[core, :, at] = (mapped * pool_scale_ref[:, at]).astype(jnp.bfloat16)

        pooled_copy.start()

    def step(n, carry):
        p = source(n)
        late = n == middle - 1
        relay(p)
        pl.when(upper & (n == 0))(release_keys)
        pl.when(n < middle - 1)(lambda: forward(source(n + 1)))
        settle(p)

        def one(i, carry):
            pl.when(n == 0)(lambda: query_arrival(i))
            pl.when(i > p)(lambda: update(i, p, False))
            pl.when(i == p)(lambda: update(i, p, True))
            pl.when((i > plane) & jnp.where(upper, n == reach, i == p))(lambda: give_back(i))
            return carry

        lax.fori_loop(jnp.where(p > plane, p, plane), planes, one, 0)
        pl.when(upper & (n == middle - 1))(release_values)

        @pl.when(late)
        def _():
            for m in range(middle, planes):
                forward(source(m))

        return carry

    forward(plane)
    loads[4].wait()
    loads[5].wait()
    theirs = pl.ds(pl.multiple_of((1 - core) * half, half), half)
    shared = [copy(outs.at[n, :, theirs], foreign.at[n], e_send.at[2 + n], e_recv.at[2 + n], sibling) for n in range(2)]
    start_all(shared)
    lax.fori_loop(0, planes, step, 0)

    def serve(i, carry):
        query_arrival(i)

        def earlier(p, carry):
            update(i, p, False)
            return carry

        lax.fori_loop(0, i, earlier, 0)
        update(i, i, True)
        give_back(i)
        return carry

    lax.fori_loop(0, plane, serve, 0)
    give_back(plane)
    pool()

    chunks = half // (2 * LANES)

    def chunk_columns(c):
        return pl.ds(pl.multiple_of(c * 2 * LANES, 2 * LANES), 2 * LANES)

    def home_columns(c):
        return pl.ds(pl.multiple_of(core * half + c * 2 * LANES, 2 * LANES), 2 * LANES)

    for n in range(2):
        arrival(foreign.at[n], e_recv.at[2 + n])

    def pool_part(c, carry):
        at = chunk_columns(c)
        whole[:, at] = jnp.dot(pooled[core], outs[0, :, home_columns(c)], preferred_element_type=jnp.float32)
        return carry

    def pool_rest(c, carry):
        at = chunk_columns(c)
        r = jnp.dot(pooled[1 - core], foreign[0, :, at], preferred_element_type=jnp.float32)
        whole[:, at] = whole[:, at] + r
        return carry

    lax.fori_loop(0, chunks, pool_part, 0)
    arrival(pooled.at[1 - core], e_recv.at[0])
    lax.fori_loop(0, chunks, pool_rest, 0)

    def pass_on(l):
        held = attended.at[core, :, columns(l)]
        return copy(held, held, p_send.at[l], p_recv.at[l], sibling)

    for p in served:
        for x in range(2):
            l = kept(p, x)
            pl.when(away(p, x, side))(lambda: arrival(attended.at[core, :, columns(l)], o_recv.at[l]))
            pass_on(l).start()

    def retain(c, carry):
        at = chunk_columns(c)
        r = jnp.dot(attended[core], outs[1, :, home_columns(c)], preferred_element_type=jnp.float32)
        whole[:, at] = whole[:, at] + r
        return carry

    lax.fori_loop(0, chunks, retain, 0)
    for l in range(planes):
        arrival(attended.at[1 - core, :, columns(l)], p_recv.at[l])

    def add(c, carry):
        at = chunk_columns(c)
        r = jnp.dot(attended[1 - core], foreign[1, :, at], preferred_element_type=jnp.float32)
        whole[:, at] = whole[:, at] + r
        return carry

    lax.fori_loop(0, chunks, add, 0)

    def square_rows(n, carry):
        at = pl.ds(pl.multiple_of(n * SUB_ROWS, SUB_ROWS), SUB_ROWS)
        mixed = whole[at, :]
        square = mixed * mixed
        row_sums[core, at, :] = functools.reduce(
            jnp.add, [square[:, c : c + LANES] for c in range(0, half, LANES)]
        )
        return carry

    lax.fori_loop(0, rows // SUB_ROWS, square_rows, 0)
    sums = copy(row_sums.at[core], row_sums.at[core], e_send.at[1], e_recv.at[1], sibling)
    sums.start()
    arrival(row_sums.at[1 - core], e_recv.at[1])

    def out_copy(n):
        at = pl.ds(pl.multiple_of(n * SUB_ROWS, SUB_ROWS), SUB_ROWS)
        return pltpu.make_async_copy(finished_rows.at[at, :], out_ref.at[at, :], f_sem.at[n])

    def finish_rows(n, carry):
        at = pl.ds(pl.multiple_of(n * SUB_ROWS, SUB_ROWS), SUB_ROWS)
        total = jnp.sum(row_sums[0, at, :] + row_sums[1, at, :], axis=1, keepdims=True)
        out_inverse = lax.rsqrt(total / width + epsilon)
        finished_rows[at, :] = (whole[at, :] * out_inverse * final_gain_ref[...]).astype(jnp.bfloat16)
        out_copy(n).start()
        return carry

    lax.fori_loop(0, rows // SUB_ROWS, finish_rows, 0)

    for p in served:
        for x in range(2):
            waited = crossing(p)
            left = (
                (lambda: query_copy(p, x).wait_send(), waited & upper, side),
                (lambda: wait_all(tensor_copies(0, p, x)), waited & upper, 0),
                (lambda: wait_all(tensor_copies(1, p, x)), False, 1),
            )
            for action, done, c in left:
                pl.when(away(p, x, c) & jnp.logical_not(done))(action)
    for p in range(planes):
        for x in range(2):
            for h in range(PIECES):
                for c in onward(p, x, h):
                    c.wait_send()
                beside(p, x, h).wait_send()
        pl.when(away(p, core, maker))(lambda: finished(p).wait_send())
    for c in [*swaps, *shared, rim_copy, pooled_copy, sums] + [pass_on(l) for l in range(planes)]:
        c.wait_send()
    for n in range(rows // SUB_ROWS):
        out_copy(n).wait()


def layer(
    tokens, input_gain, query_weight, key_weight, value_weight, pool_in_weight, log_gates,
    pool_weight, pool_scale, attention_out, pooling_out, final_gain,
):
    rows, half = tokens.shape
    width, inner = query_weight.shape
    planes = log_gates.shape[0]
    head_size = pool_weight.shape[1]
    blocks = lax.axis_size("sp")
    dma = pltpu.SemaphoreType.DMA
    tile = lambda *shape: pltpu.VMEM(shape, jnp.bfloat16)
    wide = lambda *shape: pltpu.VMEM(shape, jnp.float32)
    near = pl.BlockSpec(memory_space=pltpu.VMEM)
    away = pl.BlockSpec(memory_space=pl.ANY)
    pairs = blocks * (blocks + 1) // 2
    return pl.pallas_call(
        layer_kernel,
        out_shape=jax.ShapeDtypeStruct((rows, half), jnp.bfloat16),
        in_specs=[away, near, away, away, away, away, near, near, near, away, away, near],
        out_specs=away,
        scratch_shapes=[
            tile(rows, half), tile(rows, half), tile(4, width, inner), tile(2, inner, width), tile(2, rows, half), wide(2, rows, LANES),
            wide(rows, LANES), tile(3, rows, inner), wide(3, rows, inner), tile(WINDOW_MAX, inner), tile(rows, inner),
            wide(WINDOW_MAX + rows, head_size), tile(2, rows, inner), wide(rows, half),
            tile(2, inner, half), wide(2, rows, LANES),
            tile(2, blocks * rows, 2 * head_size), wide(*log_gates.shape), wide(1, blocks * rows),
            tile(planes, rows, head_size), tile(planes, rows, head_size), tile(2, rows, inner),
            wide(planes, rows, 2 * head_size), wide(planes, rows, LANES),
            dma((7,)), dma((rows // SUB_ROWS,)), dma((3,)), dma((3,)), dma((4,)), dma((4,)), dma((planes,)), dma((planes,)), dma, dma,
            dma((planes,)), dma((planes,)),
            dma((2, planes, PIECES)), dma((2 * planes, PIECES)),
            dma((2 * planes, PIECES)), dma((2 * planes, PIECES)),
            dma((2 * planes, PIECES)), dma((2 * planes, PIECES)),
            dma((2 * planes, PIECES)), dma((2 * planes, PIECES)),
            dma((planes,)), dma((planes,)),
        ],
        compiler_params=pltpu.CompilerParams(
            collective_id=0, has_side_effects=True, vmem_limit_bytes=56 * 2**20
        ),
        cost_estimate=pl.CostEstimate(
            flops=4 * pairs * rows * rows * head_size + 12 * rows * width * inner,
            bytes_accessed=12 * width * inner,
            transcendentals=pairs * rows * rows,
        ),
    )(
        tokens, input_gain, query_weight, key_weight, value_weight, pool_in_weight, log_gates,
        pool_weight, pool_scale.reshape(1, -1), attention_out, pooling_out, final_gain.reshape(1, -1),
    )


def ring_attend(query, keys, values, log_gates):
    tok_rows = query.shape[0]
    heads = log_gates.shape[0]
    head_size = query.shape[1] // heads
    devices = lax.axis_size("sp")
    side = 1
    while (2 * side) ** 2 <= devices and devices % (2 * side) == 0:
        side = 2 * side
    planes = devices // side
    sequence_index = lax.axis_index("sp")
    plane = sequence_index // side
    seat = sequence_index % side
    pair = jnp.concatenate([keys, values], axis=1)
    pairs = [pair]
    for _ in range(1, planes):
        pairs.append(passed_along(pairs[-1], "sp", side))
    queries = jnp.stack([query] + [swapped(query, "sp", g) for g in range(1, side)])
    seats = seat ^ jnp.arange(side, dtype=jnp.int32)
    starts = jnp.stack(
        [
            lax.dynamic_slice_in_dim(log_gates, (plane * side + (seat ^ g)) * tok_rows, 1, 1)[:, 0]
            for g in range(side)
        ]
    ).reshape(-1)
    state = None
    for k in range(planes):
        source = jnp.maximum(sequence_index - k * side, seat)
        gates = lax.dynamic_slice_in_dim(log_gates, source * tok_rows, tok_rows, 1)
        if k == 0:
            mode = (seats > seat).astype(jnp.int32)
        else:
            mode = jnp.full((side,), plane >= k, jnp.int32)
        state = attend_step(
            mode, starts, queries, pairs[k], gates, state, k == planes - 1, head_size
        )
    partial, level = state
    level = level[:, :, :heads]
    shares = [partial[0]] + [swapped(partial[g], "sp", g) for g in range(1, side)]
    tall = jnp.transpose(level, (0, 2, 1))
    levels = jnp.stack([tall[0]] + [swapped(tall[g], "sp", g) for g in range(1, side)])
    portion = jnp.exp2(levels - jnp.max(levels, axis=0, keepdims=True))
    portion = portion / jnp.sum(portion, axis=0, keepdims=True)
    portion = jnp.transpose(portion, (0, 2, 1))
    attended = 0.0
    for g in range(side):
        attended = attended + shares[g].astype(jnp.float32) * jnp.repeat(portion[g], head_size, axis=1)
    return attended.astype(jnp.bfloat16)


def gathered(block, axis):
    if lax.axis_size(axis) != 2:
        return lax.all_gather(block, axis, axis=1, tiled=True)
    other = swapped(block, axis, 1)
    lower = lax.axis_index(axis) == 0
    return jnp.concatenate([jnp.where(lower, block, other), jnp.where(lower, other, block)], axis=1)


def body(
    tokens,
    input_gain,
    query_weight,
    key_weight,
    value_weight,
    pool_in_weight,
    log_gates,
    pool_weight,
    pool_scale,
    attention_out,
    pooling_out,
    final_gain,
):
    tok_rows = tokens.shape[0]
    width = query_weight.shape[0]
    groups = pool_weight.shape[0]
    head_size = pool_weight.shape[1]
    heads = log_gates.shape[0]
    attention_width = query_weight.shape[1]
    pool_width = pool_in_weight.shape[1]
    devices = lax.axis_size("sp")
    shards = lax.axis_size("tp")
    sequence_index = lax.axis_index("sp")
    first_row = sequence_index * tok_rows
    if shards == 2 and groups % 4 == 0 and heads % 2 == 0 and devices == 4 * heads and attention_width == pool_width:
        return layer(
            tokens, input_gain, query_weight, key_weight, value_weight, pool_in_weight, log_gates,
            pool_weight, pool_scale, attention_out, pooling_out, final_gain,
        )

    part = gathered(tokens, "tp")
    gain_part = gathered(input_gain.reshape(1, -1), "tp")
    widened = part.astype(jnp.float32)
    scaled = (widened * gain_part.astype(jnp.float32)).astype(jnp.bfloat16)

    def product(weight):
        return jnp.dot(scaled, weight, preferred_element_type=jnp.float32)

    inverse = lax.rsqrt(jnp.sum(widened * widened, axis=1) / width + epsilon)[:, None]
    keys = (product(key_weight) * inverse).astype(jnp.bfloat16)
    values = (product(value_weight) * inverse).astype(jnp.bfloat16)
    query = (product(query_weight) * (inverse * (LOG2E * head_size ** (-0.5)))).astype(jnp.bfloat16)
    pool_input = (product(pool_in_weight) * inverse).astype(jnp.bfloat16)
    rim = passed_along(pool_input[tok_rows - (WINDOW_MAX - 1) :], "sp", 1)

    attended = ring_attend(query, keys, values, log_gates)

    extended = jnp.concatenate([rim, pool_input], axis=0).astype(jnp.float32)
    column = jnp.arange(pool_width, dtype=jnp.int32)
    group_number = lax.axis_index("tp") * groups + column // head_size
    window = jnp.left_shift(jnp.full((pool_width,), 2, jnp.int32), group_number % 4)
    sums = extended
    span = 1
    chosen = jnp.zeros((tok_rows, pool_width), jnp.float32)
    for _ in range(4):
        sums = sums[span:] + sums[:-span]
        span = span * 2
        offset_rows = WINDOW_MAX - span
        chosen = jnp.where(window[None, :] == span, sums[offset_rows : offset_rows + tok_rows], chosen)
    element_locations = first_row + jnp.arange(tok_rows, dtype=jnp.int32)
    counts = jnp.minimum(window[None, :], element_locations[:, None] + 1).astype(jnp.float32)
    departure = (chosen / counts - pool_input.astype(jnp.float32)).astype(jnp.bfloat16)
    mapped = jnp.concatenate(
        [
            jnp.dot(
                departure[:, g * head_size : (g + 1) * head_size],
                pool_weight[g],
                preferred_element_type=jnp.float32,
            )
            for g in range(groups)
        ],
        axis=1,
    )
    pooled = (mapped * pool_scale).astype(jnp.bfloat16)
    pooled_part = jnp.dot(pooled, pooling_out, preferred_element_type=jnp.float32)
    whole = jnp.dot(attended, attention_out, preferred_element_type=jnp.float32) + pooled_part
    if shards == 2:
        half = width // 2
        lower = lax.axis_index("tp") == 0
        sent = jnp.where(lower, whole[:, half:], whole[:, :half]).astype(jnp.bfloat16)
        kept = jnp.where(lower, whole[:, :half], whole[:, half:])
        mixed = kept + swapped(sent, "tp", 1).astype(jnp.float32)
        squares = jnp.sum(mixed * mixed, axis=1)
        squares = squares + swapped(squares, "tp", 1)
    else:
        mixed = lax.psum_scatter(
            whole.astype(jnp.bfloat16), "tp", scatter_dimension=1, tiled=True
        ).astype(jnp.float32)
        squares = lax.psum(jnp.sum(mixed * mixed, axis=1), "tp")
    out_inverse = lax.rsqrt(squares / width + epsilon)
    return (mixed * out_inverse[:, None] * final_gain[None, :]).astype(jnp.bfloat16)


def solution(mesh):
    return jax.shard_map(
        body,
        mesh=mesh,
        in_specs=(
            P("sp", "tp"),
            P("tp"),
            P(None, "tp"),
            P(None, "tp"),
            P(None, "tp"),
            P(None, "tp"),
            P("tp", None),
            P("tp", None, None),
            P("tp"),
            P("tp", None),
            P("tp", None),
            P("tp"),
        ),
        out_specs=P("sp", "tp"),
        check_vma=False,
    )
```
